32 devices in a mesh: sp: 8 (over z, x), tp: 4 (over y, core).
Axes of the slice: x: 2, y: 2, z: 4, core: 2. Of those that a mesh axis runs over, the one named last changes fastest.
Arguments:
- resid: bfloat16 [2048, 4096], P('sp'), may hold values from -6 to 6
- pool_in: bfloat16 [2048, 1024], P('sp', 'tp'), may hold values from -6 to 6
- pool_mix: bfloat16 [4, 256, 256], P('tp'), may hold values from -0.375 to 0.375
- pool_gain: float32 [1024], P('tp'), may hold values from 0.1 to 1.9
- out_proj: bfloat16 [1024, 4096], P('tp'), may hold values from -0.1875 to 0.1875
- norm_gain: float32 [4096], replicated, may hold values from 0.1 to 1.9
- w_gate: bfloat16 [8, 4096, 1024], P('sp', None, 'tp'), may hold values from -0.09375 to 0.09375
- w_up: bfloat16 [8, 4096, 1024], P('sp', None, 'tp'), may hold values from -0.09375 to 0.09375
- w_down: bfloat16 [8, 1024, 4096], P('sp', 'tp'), may hold values from -0.1875 to 0.1875
- routes: int32 [2048, 2], P('sp'), may hold values from 0 to 7, all different within a row; in each aligned block of 64 rows (0 to 63, 64 to 127, ...) at most 32 rows name the same one
- route_weight: float32 [2048, 2], P('sp'), may hold values from 0.25 to 2.5
Outputs:
- layer_out: bfloat16 [2048, 4096], P(('sp', 'tp'))
The draws below stay inside these ranges and needn't reach their ends.
Inputs may be any that keep to these rules, and one draw needn't show every extreme that they name: `routes`: in each aligned block of 64 tokens no expert is named by more than 32 of the block's rows, and the two experts of a token differ.
All inputs are finite; a program needn't handle non-finite values.
Results may differ from the reference program's by a relative error of at most 0.015.
Values may be sent and summed in bfloat16 or wider, within the bound.
A program may use at most 128 MiB of HBM per device.

```python
import math
import jax
import jax.numpy as jnp
import numpy as np
from jax import lax

D = 4096
GROUPS = 4
PCH = 256
POOLW = 1024
FF = 1024
FF_PART = 256
TOP = 2
TOK_SUB = 64
TOKENS = 2048
EXPERTS = 8
CAP = 32
N_TP = 4


def levels(key, extent, pieces, smallest, top_value):
    def one(axis_at, blocks):
        steps = jax.random.uniform(jax.random.fold_in(jax.random.fold_in(key, 6), axis_at), (blocks,), jnp.float32, smallest / len(pieces), top_value / len(pieces))
        return jnp.repeat(jnp.exp(steps), extent[axis_at] // blocks).reshape((-1,) + (1,) * (len(extent) - axis_at - 1))

    factor_of = one(*pieces[0])
    for cut in pieces[1:]:
        factor_of = factor_of * one(*cut)
    return factor_of


def shared_out(stream_key, own, number, rows, count, top, limit, lean):
    order = jax.random.permutation(stream_key, count)
    crowded, common = portions_of(count, rows * top, limit, lean, True), portions_of(count, rows * top, limit, lean, False)
    places = jnp.arange(count)

    def named(tallies, turn):
        used = int((tallies > 0).sum())
        fixed = max(1, used // 4)
        passed = fixed + (places - fixed + turn * (used - fixed)) % max(1, count - fixed)
        return jnp.zeros((count,), jnp.int32).at[order[jnp.where(places < fixed, places, passed)]].set(jnp.asarray(tallies, jnp.int32))

    tallies = jnp.where(number % 4 == 0, named(crowded, number // 4), named(common, number - number // 4 - 1))
    mixed = jax.random.permutation(jax.random.fold_in(own, 3), count)
    giver, taker = mixed[0:count // 2 * 2:2], mixed[1:count // 2 * 2:2]
    room = jnp.minimum(tallies[giver] - 1, limit - tallies[taker]) // 2
    room = jnp.where((giver == order[0]) | (taker == order[0]) | (tallies[taker] == 0), 0, jnp.maximum(room, 0))
    passed = jax.random.randint(jax.random.fold_in(own, 4), (count // 2,), 0, 1 << 20) % (room + 1)
    tallies = tallies.at[giver].add(-passed).at[taker].add(passed)
    members = jnp.searchsorted(jnp.cumsum(tallies), jnp.arange(rows * top), side="right").astype(jnp.int32)
    listing = members.reshape(top, rows).T
    listing = listing[jax.random.permutation(jax.random.fold_in(own, 1), rows)]
    turn = jax.random.randint(jax.random.fold_in(own, 2), (rows, 1), 0, top)
    return jnp.take_along_axis(listing, (jnp.arange(top)[None, :] + turn) % top, axis=1)


def portions_of(count, total, limit, slope, full):
    portions = [(1 << 20) // math.isqrt(grade ** slope) + 1 for grade in range(1, count + 1)]
    largest = limit if full else min(limit, max(-(-total // count), total * portions[0] // sum(portions)))
    least = 1 if total - largest >= count - 1 else 0
    holding, rest = [largest] + [least] * (count - 1), total - largest - least * (count - 1)
    while rest > 0:
        candidates = [i for i in range(1, count) if holding[i] < largest] or [i for i in range(1, count) if holding[i] < limit]
        pool, left = sum([portions[i] for i in candidates]), rest
        for i in candidates:
            more = min(limit - holding[i], max(1, left * portions[i] // pool), rest)
            holding[i] = holding[i] + more
            rest = rest - more
    return np.array(holding)


def noise(own_key, shape, deviation, limit, pieces=(), held_as=jnp.bfloat16):
    array = deviation * jax.random.normal(own_key, shape, jnp.float32)
    if pieces:
        array = array * levels(own_key, shape, pieces, -0.22, 0.18)
    return jnp.clip(array, -limit, limit).astype(held_as)


def setup_inputs(seed: int = 0) -> dict:
    streams_of = jax.random.split(jax.random.key(seed), 12)
    resid = noise(streams_of[0], (TOKENS, D), 1.0, 6.0, ((0, 8),))
    pool_in = noise(streams_of[1], (TOKENS, POOLW), 1.0, 6.0, ((0, 8), (1, 4)))
    pool_mix = noise(streams_of[2], (GROUPS, PCH, PCH), PCH ** -0.5, 0.375, ((0, 4),))
    pool_gain = jnp.clip(1.0 + 0.18 * jax.random.normal(streams_of[3], (POOLW,), jnp.float32), 0.1, 1.9)
    out_proj = noise(streams_of[4], (POOLW, D), POOLW ** -0.5, 0.1875, ((0, 4),))
    norm_gain = jnp.clip(1.0 + 0.18 * jax.random.normal(streams_of[5], (D,), jnp.float32), 0.1, 1.9)
    w_gate = noise(streams_of[6], (EXPERTS, D, FF), D ** -0.5, 0.09375, ((0, 8), (2, 4)))
    w_up = noise(streams_of[7], (EXPERTS, D, FF), D ** -0.5, 0.09375, ((0, 8), (2, 4)))
    w_down = noise(streams_of[8], (EXPERTS, FF, D), FF ** -0.5, 0.1875, ((0, 8), (1, 4)))
    routes_keys = jax.random.split(jax.random.fold_in(streams_of[9], 1), TOKENS // TOK_SUB)
    routes_turns = jax.random.permutation(jax.random.fold_in(streams_of[9], 3), TOKENS // TOK_SUB)
    routes = jax.vmap(lambda own, number: shared_out(jax.random.fold_in(streams_of[9], 2), own, number, TOK_SUB, EXPERTS, TOP, CAP, 2))(routes_keys, routes_turns).reshape((TOKENS, TOP))
    route_weight = jnp.clip(jnp.exp(math.log(2.5) - 2.3025851 * jax.random.uniform(streams_of[10], (TOKENS, TOP), jnp.float32) ** levels(streams_of[10], (TOKENS, TOP), ((0, 8),), -0.2, 0.2)), 0.25, 2.5)
    return {"resid": resid, "pool_in": pool_in, "pool_mix": pool_mix, "pool_gain": pool_gain, "out_proj": out_proj, "norm_gain": norm_gain, "w_gate": w_gate, "w_up": w_up, "w_down": w_down, "routes": routes, "route_weight": route_weight}


EPS = 1e-06

def rounded(value):
    return lax.optimization_barrier(value.astype(jnp.bfloat16)).astype(jnp.float32)

def window_diff(block, width):
    row_count = block.shape[0]
    data = block.astype(jnp.float32)
    padded = jnp.concatenate([jnp.zeros((width - 1, data.shape[1]), jnp.float32), data], axis=0)
    total = jnp.zeros_like(data)
    for offset in range(width):
        total = total + padded[width - 1 - offset:width - 1 - offset + row_count]
    counted = jnp.minimum(jnp.arange(1, row_count + 1, dtype=jnp.float32), float(width))
    return (total / counted[:, None] - data).astype(jnp.bfloat16)

def reference(resid, pool_in, pool_mix, pool_gain, out_proj, norm_gain, w_gate, w_up, w_down, routes, route_weight):
    proj = jnp.zeros((TOKENS, D), jnp.float32)
    for group in range(GROUPS):
        lower = group * PCH
        diff = window_diff(pool_in[:, lower:lower + PCH], 2 ** (group + 1))
        pooled = (jnp.dot(diff, pool_mix[group], preferred_element_type=jnp.float32) * pool_gain[lower:lower + PCH]).astype(jnp.bfloat16)
        proj = proj + rounded(jnp.dot(pooled, out_proj[lower:lower + PCH], preferred_element_type=jnp.float32))
    proj = rounded(proj)
    mixed = resid.astype(jnp.float32) + proj
    scale = lax.rsqrt(lax.optimization_barrier(jnp.mean(mixed * mixed, axis=1, keepdims=True)) + EPS)
    normed = (mixed * scale * norm_gain).astype(jnp.bfloat16)
    normed_ext = jnp.concatenate([normed, jnp.zeros((1, D), jnp.bfloat16)], axis=0)
    flat_expert = routes.reshape(-1)
    flat_weight = route_weight.reshape(-1)
    flat_token = (jnp.arange(TOKENS * TOP, dtype=jnp.int32) // TOP).astype(jnp.int32)
    most = TOKENS // TOK_SUB * CAP

    def one_expert(total, expert):
        match = flat_expert == expert
        position = jnp.cumsum(match.astype(jnp.int32)) - 1
        slot = jnp.where(match, position, most).astype(jnp.int32)
        owner = jnp.full((most + 1,), TOKENS, jnp.int32).at[slot].set(flat_token)[:most]
        weight = jnp.zeros((most + 1,), jnp.float32).at[slot].set(flat_weight)[:most]
        inputs = normed_ext[owner]
        gate = jnp.dot(inputs, w_gate[expert], preferred_element_type=jnp.float32)
        upper = jnp.dot(inputs, w_up[expert], preferred_element_type=jnp.float32)
        hidden = (jax.nn.silu(gate) * upper).astype(jnp.bfloat16)
        down = w_down[expert]
        result = jnp.zeros((most, D), jnp.float32)
        for block in range(N_TP):
            lower = block * FF_PART
            result = result + rounded(jnp.dot(hidden[:, lower:lower + FF_PART], down[lower:lower + FF_PART], preferred_element_type=jnp.float32))
        total = total.at[owner].add(result * weight[:, None])
        return (total, None)
    moe, unused = lax.scan(one_expert, jnp.zeros((TOKENS + 1, D), jnp.float32), jnp.arange(EXPERTS, dtype=jnp.int32))
    return (mixed + moe[:TOKENS]).astype(jnp.bfloat16)
```

```python
import functools

import jax
import jax.numpy as jnp
from jax import lax
from jax.experimental import pallas as pl
from jax.experimental.pallas import tpu as pltpu
from jax.sharding import PartitionSpec as P

GROUPS = 4


EPS = 1e-06


def shifted(x, axis, by):
    count = lax.axis_size(axis)
    pairs = [(i, i + by) for i in range(count) if 0 <= i + by < count]
    return lax.ppermute(x, axis, pairs)


def rounded(value):
    return lax.optimization_barrier(value.astype(jnp.bfloat16)).astype(jnp.float32)


def group_diff(pool_in):
    row_count = pool_in.shape[0]
    reach = 2**GROUPS
    before = shifted(pool_in[row_count - reach :], "sp", 1)
    joined = jnp.concatenate([before, pool_in], axis=0).astype(jnp.float32)
    running = jnp.cumsum(joined, axis=0)
    width = jnp.left_shift(jnp.int32(2), lax.axis_index("tp"))
    lagged = lax.dynamic_slice_in_dim(running, reach - width, row_count, 0)
    total = running[reach:] - lagged
    place = lax.axis_index("sp") * row_count + jnp.arange(row_count, dtype=jnp.int32) + 1
    counted = jnp.minimum(place, width).astype(jnp.float32)
    return (total / counted[:, None] - joined[reach:]).astype(jnp.bfloat16)


def normalize(mixed, norm_gain):
    scale = lax.rsqrt(jnp.mean(mixed * mixed, axis=1, keepdims=True) + EPS)
    return (mixed * scale * norm_gain).astype(jnp.bfloat16)


def slot_plan(route_rows, blocks, capacity, experts):
    row_count, choose = route_rows.shape
    flat_routes = route_rows.reshape(blocks, row_count // blocks * choose)
    onehot = (
        flat_routes[:, :, None] == jnp.arange(experts, dtype=jnp.int32)[None, None, :]
    ).astype(jnp.int32)
    earlier = jnp.cumsum(onehot, axis=1) - onehot
    position = jnp.sum(earlier * onehot, axis=2)
    block_ids = jnp.arange(blocks, dtype=jnp.int32)[:, None]
    return (flat_routes * (blocks * capacity) + block_ids * capacity + position).reshape(-1)


def fill_slots(normed, targets, slot_count):
    row_count, width = normed.shape
    slots = jnp.arange(slot_count, dtype=jnp.int32)[:, None, None]
    picks = jnp.sum((targets.reshape(row_count, -1)[None] == slots).astype(jnp.bfloat16), axis=2)
    return jnp.dot(picks, normed, preferred_element_type=jnp.float32).astype(normed.dtype)


def collect(returned, targets, weights):
    row_count, choose = weights.shape
    slots = jnp.arange(returned.shape[0], dtype=jnp.int32)[None, None, :]
    chosen = targets.reshape(row_count, choose)[:, :, None] == slots
    spread = jnp.sum(jnp.where(chosen, weights[:, :, None], 0.0), axis=1)
    head = lax.reduce_precision(spread, 8, 7)
    tail = spread - head
    both = jnp.concatenate([head, tail], axis=0).astype(jnp.bfloat16)
    product = jnp.dot(both, returned, preferred_element_type=jnp.float32)
    return product[:row_count] + product[row_count:]


def expert_part(inputs, w_gate, w_up, w_down):
    gate = jnp.dot(inputs, w_gate[0], preferred_element_type=jnp.float32)
    upper = jnp.dot(inputs, w_up[0], preferred_element_type=jnp.float32)
    hidden = (jax.nn.silu(gate) * upper).astype(jnp.bfloat16)
    return jnp.dot(hidden, w_down[0], preferred_element_type=jnp.float32).astype(jnp.bfloat16)


def line_plan(z):
    first = z + 1 - 2 * (z % 2)
    second = 2 - z // 2
    third = 3 - 3 * (z // 2)
    return first, second, third


def moe_kernel(
    front, back, capacity, experts,
    rows_in, meta_in, wg_hbm, wu_hbm, wd_hbm, out,
    wg, wu, wd, rows, meta, slots, give, parts,
    mate_in, y_in, x_in, sums, line_in, home_in, last_in,
    w_sem, m_send, m_recv, r_recv, ry_send, ra_send, rb_send,
    xf_send, xf_recv, yf_send, yf_recv, mf_send, mf_recv,
    mb_send, mb_recv, yb_send, yb_recv, xb_send, xb_recv,
    zf_send, zf_recv, zh_send, zh_recv, yl_send, yl_recv,
):
    me = lax.axis_index("sp")
    tp = lax.axis_index("tp")
    z, x = me // 2, me % 2
    y, c = tp // 2, tp % 2
    C = capacity
    tokens, width = rows_in.shape
    wf, wb = width // front, width // back
    z1, z2, z3 = line_plan(z)
    mid = ((z + 1) // 2) % 2 == 1
    end = ((z + 1) // 2) % 2 == 0
    mate = (me, y * 2 + 1 - c)
    across = (me, (1 - y) * 2 + c)
    peer_expert = me + 1 - 2 * x
    beside = (peer_expert, tp)
    f32, bf16 = jnp.float32, jnp.bfloat16

    def plane(zz):
        return (zz * 2 + x, tp)

    def remote(src, dst, send, recv, to):
        return pltpu.make_async_remote_copy(
            src_ref=src, dst_ref=dst, send_sem=send, recv_sem=recv,
            device_id=to, device_id_type=pl.DeviceIdType.MESH,
        )

    def fcols(h):
        return pl.ds(pl.multiple_of(h * wf, wf), wf)

    def bcols(h):
        return pl.ds(pl.multiple_of(h * wb, wb), wb)

    def spot(xx, yy):
        return pl.ds(pl.multiple_of(c * 4 * C + xx * 2 * C + yy * C, C), C)

    def both(xx):
        return pl.ds(pl.multiple_of(c * 4 * C + xx * 2 * C, 2 * C), 2 * C)

    def half(cc):
        return pl.ds(pl.multiple_of(cc * 4 * C, 4 * C), 4 * C)

    def strip(yy):
        return pl.ds(pl.multiple_of(yy * C, C), C)

    def meta_copy(q):
        zq, yq = (z + q // 2) % 4, (y + q) % 2
        return remote(meta_in, meta.at[z, y], m_send.at[q], m_recv.at[z, y],
                      (zq * 2 + x, yq * 2 + c))

    def meta_here(zt, yt):
        remote(meta.at[zt, yt], meta.at[zt, yt], m_send.at[0], m_recv.at[zt, yt],
               mate).wait_recv()

    def dup_copy(h):
        return remote(rows_in.at[:, fcols(h)], rows.at[z, y, :, fcols(h)],
                      ry_send.at[h], r_recv.at[z, y, h], across)

    def own_copy(h, to, send):
        return remote(rows_in.at[:, fcols(h)], rows.at[z, y, :, fcols(h)],
                      send.at[z, y, h], r_recv.at[z, y, h], plane(to))

    def pass_copy(zt, yt, h, to, send):
        ref = rows.at[zt, yt, :, fcols(h)]
        return remote(ref, ref, send.at[zt, yt, h], r_recv.at[zt, yt, h], plane(to))

    def rows_here(zt, yt, h):
        ref = rows.at[zt, yt, :, fcols(h)]
        remote(ref, ref, ry_send.at[h], r_recv.at[zt, yt, h], mate).wait_recv()

    def xf_copy(zt, yt, h):
        return remote(give.at[zt, strip(yt), fcols(h)], slots.at[zt, spot(x, yt), fcols(h)],
                      xf_send.at[zt, yt, h], xf_recv.at[zt, yt, h], beside)

    def yf_copy(zt, xx, h):
        ref = slots.at[zt, spot(xx, y), fcols(h)]
        return remote(ref, ref, yf_send.at[zt, xx, h], yf_recv.at[zt, xx, h], across)

    def mf_copy(zt, h):
        ref = slots.at[zt, half(c), fcols(h)]
        return remote(ref, ref, mf_send.at[zt, h], mf_recv.at[zt, h], mate)

    def mb_copy(zt, h):
        return remote(parts.at[zt, half(1 - c), bcols(h)], mate_in.at[zt, :, bcols(h)],
                      mb_send.at[zt, h], mb_recv.at[zt, h], mate)

    def yb_copy(zt, xx, h):
        return remote(parts.at[zt, spot(xx, 1 - y), bcols(h)], y_in.at[zt, strip(xx), bcols(h)],
                      yb_send.at[zt, xx, h], yb_recv.at[zt, xx, h], across)

    def xb_copy(zt, near, h):
        if near:
            return remote(parts.at[zt, both(1 - x), bcols(h)], x_in.at[zt, :, bcols(h)],
                          xb_send.at[zt, h], xb_recv.at[zt, h], beside)
        return remote(parts.at[zt, spot(1 - x, y), bcols(h)], x_in.at[zt, strip(y), bcols(h)],
                      xb_send.at[zt, h], xb_recv.at[zt, h], beside)

    def line_copy(zt, h, to):
        return remote(sums.at[zt, y, :, bcols(h)], line_in.at[zt, :, bcols(h)],
                      zf_send.at[zt, h], zf_recv.at[zt, h], plane(to))

    def home_copy(zt, yt, side, h):
        return remote(sums.at[zt, yt, :, bcols(h)], home_in.at[side, yt, :, bcols(h)],
                      zh_send.at[side, yt, h], zh_recv.at[side, yt, h], plane(zt))

    def home_here(yt, side, h):
        ref = home_in.at[side, yt, :, bcols(h)]
        remote(ref, ref, zh_send.at[side, yt, h], zh_recv.at[side, yt, h], mate).wait_recv()

    def last_copy(h):
        return remote(sums.at[z, 1 - y, :, bcols(h)], last_in.at[:, bcols(h)],
                      yl_send.at[h], yl_recv.at[h], across)

    loads = [
        pltpu.make_async_copy(wg_hbm.at[0], wg, w_sem.at[0]),
        pltpu.make_async_copy(wu_hbm.at[0], wu, w_sem.at[1]),
        pltpu.make_async_copy(wd_hbm.at[0], wd, w_sem.at[2]),
    ]

    barrier = pltpu.get_barrier_semaphore()
    for peer in (mate, beside):
        pl.semaphore_signal(barrier, inc=1, device_id=peer,
                            device_id_type=pl.DeviceIdType.MESH)

    @pl.loop(1, 8)
    def _(q):
        zq, yq = (z + q // 2) % 4, (y + q) % 2
        pl.semaphore_signal(barrier, inc=1, device_id=(zq * 2 + x, yq * 2 + c),
                            device_id_type=pl.DeviceIdType.MESH)

    pl.semaphore_wait(barrier, 9)

    @pl.loop(1, 8)
    def _(q):
        meta_copy(q).start()

    @pl.loop(0, front)
    def _(h):
        dup_copy(h).start()
        own_copy(h, z1, ra_send).start()

        @pl.when(mid)
        def _():
            own_copy(h, z2, rb_send).start()

    for load in loads:
        load.start()
    meta[z, y] = meta_in[...]
    rows[z, y] = rows_in[...]

    def picks_of(zt, yt):
        places = meta[zt, yt, tokens:tokens + experts, :]
        level = lax.broadcasted_iota(jnp.int32, places.shape, 0)
        slot = lax.broadcasted_iota(jnp.int32, (C, tokens), 0).astype(f32)

        def one(expert):
            place = jnp.sum(jnp.where(level == expert, places, 0.0), axis=0, keepdims=True)
            return jnp.where(place[:, :tokens] == slot, 1.0, 0.0)

        return jnp.concatenate([one(me), one(peer_expert)], axis=0).astype(bf16)

    def gather(picks, zt, yt, h):
        found = jnp.dot(picks, rows[zt, yt, :, fcols(h)], preferred_element_type=f32)
        found = found.astype(bf16)
        slots[zt, spot(x, yt), fcols(h)] = found[:C]
        give[zt, strip(yt), fcols(h)] = found[C:]
        xf_copy(zt, yt, h).start()

    def arrive(zt, yt, far, onward):
        meta_here(zt, yt)
        picks = picks_of(zt, yt)

        @pl.loop(0, front)
        def _(h):
            rows_here(zt, yt, h)
            onward(h)
            gather(picks, zt, yt, h)
            if far:
                yf_copy(zt, x, h).start()

    def nothing(h):
        pass

    def complete(zt, far):
        @pl.loop(0, front)
        def _(h):
            xf_copy(zt, y, h).wait_recv()
            if far:
                yf_copy(zt, 1 - x, h).start()
            else:
                xf_copy(zt, 1 - y, h).wait_recv()
                mf_copy(zt, h).start()

        if far:
            @pl.loop(0, front)
            def _(h):
                yf_copy(zt, x, h).wait_recv()
                yf_copy(zt, 1 - x, h).wait_recv()
                mf_copy(zt, h).start()

    def compute(zt):
        @pl.loop(0, front)
        def _(h):
            mf_copy(zt, h).wait_recv()

        v = slots[zt]
        gate = jnp.dot(v, wg[...], preferred_element_type=f32)
        upper = jnp.dot(v, wu[...], preferred_element_type=f32)
        hidden = (gate * (1.0 / (1.0 + jnp.exp(-gate))) * upper).astype(bf16)

        @pl.loop(0, back)
        def _(h):
            parts[zt, :, bcols(h)] = jnp.dot(
                hidden, wd[:, bcols(h)], preferred_element_type=f32
            ).astype(bf16)
            mb_copy(zt, h).start()

    def pair_sum(zt, far):
        @pl.loop(0, back)
        def _(h):
            mb_copy(zt, h).wait_recv()
            total = (
                parts[zt, half(c), bcols(h)].astype(f32) + mate_in[zt, :, bcols(h)].astype(f32)
            )
            parts[zt, half(c), bcols(h)] = total.astype(bf16)
            if far:
                yb_copy(zt, 0, h).start()
                yb_copy(zt, 1, h).start()
            else:
                xb_copy(zt, True, h).start()

    def far_sum(zt):
        @pl.loop(0, back)
        def _(h):
            for xx in (0, 1):
                yb_copy(zt, xx, h).wait_recv()
                total = (
                    parts[zt, spot(xx, y), bcols(h)].astype(f32)
                    + y_in[zt, strip(xx), bcols(h)].astype(f32)
                )
                parts[zt, spot(xx, y), bcols(h)] = total.astype(bf16)
            xb_copy(zt, False, h).start()

    def weights_of(zt, yt):
        info = meta[zt, yt, :tokens, :]
        lane = lax.broadcasted_iota(jnp.int32, info.shape, 1)
        slot = lax.broadcasted_iota(jnp.int32, (tokens, C), 1).astype(f32)

        def one(expert):
            place = jnp.sum(jnp.where(lane == expert, info, 0.0), axis=1, keepdims=True)
            weight = jnp.sum(
                jnp.where(lane == experts + expert, info, 0.0), axis=1, keepdims=True
            )
            spread = jnp.where(place == slot, weight, 0.0)
            head = spread.astype(bf16)
            return head, (spread - head.astype(f32)).astype(bf16)

        mine, theirs = one(me), one(peer_expert)
        return jnp.concatenate([mine[0], theirs[0], mine[1], theirs[1]], axis=1)

    def blend(spread, zt, yt, h):
        mine = parts[zt, spot(x, yt), bcols(h)]
        theirs = x_in[zt, strip(yt), bcols(h)]
        pair = jnp.concatenate([mine, theirs, mine, theirs], axis=0)
        return jnp.dot(spread, pair, preferred_element_type=f32)

    def near_back(zt, side):
        here = weights_of(zt, y)
        there = weights_of(zt, 1 - y)

        @pl.loop(0, back)
        def _(h):
            xb_copy(zt, True, h).wait_recv()
            sums[zt, 1 - y, :, bcols(h)] = blend(there, zt, 1 - y, h).astype(bf16)
            home_copy(zt, 1 - y, side, h).start()
            total = blend(here, zt, y, h)

            @pl.when(mid)
            def _():
                line_copy(zt, h, z1).wait_recv()
                sums[zt, y, :, bcols(h)] = (
                    total + line_in[zt, :, bcols(h)].astype(f32)
                ).astype(bf16)

            @pl.when(end)
            def _():
                sums[zt, y, :, bcols(h)] = total.astype(bf16)

            home_copy(zt, y, side, h).start()

    def far_back(zt):
        here = weights_of(zt, y)

        @pl.loop(0, back)
        def _(h):
            xb_copy(zt, False, h).wait_recv()
            total = blend(here, zt, y, h)

            @pl.when(mid)
            def _():
                line_copy(zt, h, z1).wait_recv()
                sums[zt, y, :, bcols(h)] = (
                    total + line_in[zt, :, bcols(h)].astype(f32)
                ).astype(bf16)
                line_copy(zt, h, z2).start()

            @pl.when(end)
            def _():
                sums[zt, y, :, bcols(h)] = total.astype(bf16)
                line_copy(zt, h, z1).start()

    def own_back():
        here = weights_of(z, y)
        there = weights_of(z, 1 - y)

        @pl.loop(0, back)
        def _(h):
            xb_copy(z, True, h).wait_recv()
            sums[z, 1 - y, :, bcols(h)] = blend(there, z, 1 - y, h).astype(bf16)
            out[:, bcols(h)] = blend(here, z, y, h)

    own_picks = picks_of(z, y)

    @pl.loop(0, front)
    def _(h):
        gather(own_picks, z, y, h)

    def dup_on(h):
        pass_copy(z, 1 - y, h, z1, ra_send).start()

        @pl.when(mid)
        def _():
            pass_copy(z, 1 - y, h, z2, rb_send).start()

    arrive(z, 1 - y, False, dup_on)

    def first_on(h):
        @pl.when(mid)
        def _():
            pass_copy(z1, y, h, z2, rb_send).start()

    arrive(z1, y, False, first_on)

    @pl.when(mid)
    def _():
        arrive(z2, y, False, lambda h: pass_copy(z2, y, h, z1, ra_send).start())

    complete(z, False)
    for load in loads:
        load.wait()
    compute(z)
    arrive(z1, 1 - y, False, nothing)

    @pl.when(mid)
    def _():
        arrive(z2, 1 - y, False, nothing)

    pair_sum(z, False)
    complete(z1, False)
    compute(z1)
    pair_sum(z1, False)

    @pl.when(end)
    def _():
        arrive(z2, y, True, nothing)

    own_back()

    @pl.when(end)
    def _():
        near_back(z1, 0)
        complete(z2, True)

    @pl.when(mid)
    def _():
        complete(z2, False)

    compute(z2)

    @pl.when(end)
    def _():
        pair_sum(z2, True)

    @pl.when(mid)
    def _():
        pair_sum(z2, False)

    def third_on(h):
        @pl.when(mid)
        def _():
            pass_copy(z3, y, h, z1, ra_send).start()

    arrive(z3, y, True, third_on)

    @pl.when(end)
    def _():
        far_sum(z2)

    complete(z3, True)
    compute(z3)
    pair_sum(z3, True)

    @pl.when(end)
    def _():
        far_back(z2)

    far_sum(z3)

    @pl.when(mid)
    def _():
        near_back(z2, 1)

    far_back(z3)

    @pl.when(mid)
    def _():
        near_back(z1, 0)

    @pl.loop(0, back)
    def _(h):
        home_here(1 - y, 0, h)
        total = (
            sums[z, 1 - y, :, bcols(h)].astype(f32) + home_in[0, 1 - y, :, bcols(h)].astype(f32)
        )

        @pl.when(mid)
        def _():
            home_here(1 - y, 1, h)
            sums[z, 1 - y, :, bcols(h)] = (
                total + home_in[1, 1 - y, :, bcols(h)].astype(f32)
            ).astype(bf16)

        @pl.when(end)
        def _():
            sums[z, 1 - y, :, bcols(h)] = total.astype(bf16)

        last_copy(h).start()

    @pl.loop(0, back)
    def _(h):
        home_here(y, 0, h)
        total = out[:, bcols(h)] + home_in[0, y, :, bcols(h)].astype(f32)

        @pl.when(mid)
        def _():
            home_here(y, 1, h)
            out[:, bcols(h)] = total + home_in[1, y, :, bcols(h)].astype(f32)

        @pl.when(end)
        def _():
            out[:, bcols(h)] = total

        last_copy(h).wait_recv()
        out[:, bcols(h)] += last_in[:, bcols(h)].astype(f32)

    meta_here(z3, 1 - y)

    @pl.when(end)
    def _():
        meta_here(z2, 1 - y)

    @pl.loop(1, 8)
    def _(q):
        meta_copy(q).wait_send()

    @pl.loop(0, front)
    def _(h):
        dup_copy(h).wait_send()
        own_copy(h, z1, ra_send).wait_send()
        pass_copy(z, 1 - y, h, z1, ra_send).wait_send()
        for zt in (z, z1):
            for yt in (0, 1):
                xf_copy(zt, yt, h).wait_send()
        xf_copy(z2, y, h).wait_send()
        xf_copy(z3, y, h).wait_send()
        for zt in (z, z1, z2, z3):
            mf_copy(zt, h).wait_send()
        yf_copy(z3, 0, h).wait_send()
        yf_copy(z3, 1, h).wait_send()

        @pl.when(mid)
        def _():
            own_copy(h, z2, rb_send).wait_send()
            pass_copy(z, 1 - y, h, z2, rb_send).wait_send()
            pass_copy(z1, y, h, z2, rb_send).wait_send()
            pass_copy(z2, y, h, z1, ra_send).wait_send()
            pass_copy(z3, y, h, z1, ra_send).wait_send()
            xf_copy(z2, 1 - y, h).wait_send()

        @pl.when(end)
        def _():
            yf_copy(z2, 0, h).wait_send()
            yf_copy(z2, 1, h).wait_send()

    @pl.loop(0, back)
    def _(h):
        for zt in (z, z1, z2, z3):
            mb_copy(zt, h).wait_send()
        xb_copy(z, True, h).wait_send()
        xb_copy(z1, True, h).wait_send()
        xb_copy(z3, False, h).wait_send()
        yb_copy(z3, 0, h).wait_send()
        yb_copy(z3, 1, h).wait_send()
        line_copy(z3, h, z1).wait_send()
        home_copy(z1, 0, 0, h).wait_send()
        home_copy(z1, 1, 0, h).wait_send()
        last_copy(h).wait_send()

        @pl.when(mid)
        def _():
            xb_copy(z2, True, h).wait_send()
            home_copy(z2, 0, 1, h).wait_send()
            home_copy(z2, 1, 1, h).wait_send()

        @pl.when(end)
        def _():
            xb_copy(z2, False, h).wait_send()
            yb_copy(z2, 0, h).wait_send()
            yb_copy(z2, 1, h).wait_send()
            line_copy(z2, h, z1).wait_send()


FRONT, BACK = 2, 4


def moe_exchange(normed, meta, w_gate, w_up, w_down, capacity, experts):
    tokens, width = normed.shape
    units = w_gate.shape[2]
    bf16 = jnp.bfloat16
    dma = pltpu.SemaphoreType.DMA
    C = capacity
    vmem = pltpu.VMEM
    pair = [dma((4, 2, FRONT))] * 2
    back2 = [dma((4, 2, BACK))] * 2
    back1 = [dma((4, BACK))] * 2
    return pl.pallas_call(
        functools.partial(moe_kernel, FRONT, BACK, capacity, experts),
        out_shape=jax.ShapeDtypeStruct((tokens, width), jnp.float32),
        in_specs=[pl.BlockSpec(memory_space=pltpu.VMEM)] * 2
        + [pl.BlockSpec(memory_space=pl.ANY)] * 3,
        out_specs=pl.BlockSpec(memory_space=pltpu.VMEM),
        scratch_shapes=[
            vmem((width, units), bf16),
            vmem((width, units), bf16),
            vmem((units, width), bf16),
            vmem((4, 2, tokens, width), bf16),
            vmem((4, 2) + meta.shape, jnp.float32),
            vmem((4, 8 * C, width), bf16),
            vmem((4, 2 * C, width), bf16),
            vmem((4, 8 * C, width), bf16),
            vmem((4, 4 * C, width), bf16),
            vmem((4, 2 * C, width), bf16),
            vmem((4, 2 * C, width), bf16),
            vmem((4, 2, tokens, width), bf16),
            vmem((4, tokens, width), bf16),
            vmem((2, 2, tokens, width), bf16),
            vmem((tokens, width), bf16),
            dma((3,)), dma((8,)), dma((4, 2)), dma((4, 2, FRONT)), dma((FRONT,)),
            dma((4, 2, FRONT)), dma((4, 2, FRONT)),
        ]
        + pair + pair + [dma((4, FRONT))] * 2
        + back1 + back2 + back1 + back1 + [dma((2, 2, BACK))] * 2 + [dma((BACK,))] * 2,
        compiler_params=pltpu.CompilerParams(
            collective_id=1, has_side_effects=True, vmem_limit_bytes=60 * 2**20
        ),
        cost_estimate=pl.CostEstimate(
            flops=6 * experts * 4 * C * width * units,
            bytes_accessed=3 * 2 * width * units,
            transcendentals=0,
        ),
        name="moe_exchange",
    )(normed, meta, w_gate, w_up, w_down)


def token_table(route_rows, weight_rows, experts):
    row_count = route_rows.shape[0]
    f32 = jnp.float32
    chosen = route_rows[:, :, None] == jnp.arange(experts, dtype=jnp.int32)[None, None, :]
    hit = jnp.any(chosen, axis=1)
    order = jnp.arange(row_count)
    earlier = (order[:, None] > order[None, :]).astype(jnp.bfloat16)
    place = jnp.dot(earlier, hit.astype(jnp.bfloat16), preferred_element_type=f32)
    place = jnp.where(hit, place, -1.0)
    weight = jnp.sum(jnp.where(chosen, weight_rows[:, :, None], 0.0), axis=1)
    by_token = jnp.pad(
        jnp.concatenate([place, weight], axis=1), ((0, 0), (0, 128 - 2 * experts))
    )
    by_expert = jnp.pad(place.T, ((0, 0), (0, 128 - row_count)), constant_values=-1.0)
    return jnp.concatenate([by_token, by_expert], axis=0)


def sum_kernel(count, part, out, pair_in, total, y_in, pp_send, pp_recv, y_send, y_recv):
    me = lax.axis_index("sp")
    tp = lax.axis_index("tp")
    core, y = tp % 2, tp // 2
    mate = y * 2 + (1 - core)
    across = (1 - y) * 2 + core
    pieces = count // 16
    mesh_id = pl.DeviceIdType.MESH
    barrier = pltpu.get_barrier_semaphore()
    for peer in (mate, across):
        pl.semaphore_signal(barrier, inc=1, device_id=(me, peer), device_id_type=mesh_id)
    pl.semaphore_wait(barrier, 2)

    def at(yy, c, k):
        return pl.ds(pl.multiple_of((yy * 2 + c) * count + k * 16, 16), 16)

    def piece(k):
        return pl.ds(pl.multiple_of(k * 16, 16), 16)

    def pair_copy(yy, k, place):
        return pltpu.make_async_remote_copy(
            src_ref=part.at[at(yy, 1 - core, k)], dst_ref=pair_in.at[place, piece(k)],
            send_sem=pp_send.at[place, k], recv_sem=pp_recv.at[place, k],
            device_id=(me, mate), device_id_type=mesh_id,
        )

    def far_copy(k):
        return pltpu.make_async_remote_copy(
            src_ref=total.at[piece(k)], dst_ref=y_in.at[piece(k)],
            send_sem=y_send.at[k], recv_sem=y_recv.at[k],
            device_id=(me, across), device_id_type=mesh_id,
        )

    @pl.loop(0, pieces)
    def _(k):
        pair_copy(1 - y, k, 0).start()

    @pl.loop(0, pieces)
    def _(k):
        pair_copy(y, k, 1).start()

    @pl.loop(0, pieces)
    def _(k):
        pair_copy(1 - y, k, 0).wait_recv()
        total[piece(k)] = (
            part[at(1 - y, core, k)].astype(jnp.float32)
            + pair_in[0, piece(k)].astype(jnp.float32)
        ).astype(jnp.bfloat16)
        far_copy(k).start()

    @pl.loop(0, pieces)
    def _(k):
        pair_copy(y, k, 1).wait_recv()
        far_copy(k).wait_recv()
        out[piece(k)] = (
            part[at(y, core, k)].astype(jnp.float32)
            + pair_in[1, piece(k)].astype(jnp.float32)
            + y_in[piece(k)].astype(jnp.float32)
        ).astype(jnp.bfloat16)

    @pl.loop(0, pieces)
    def _(k):
        pair_copy(1 - y, k, 0).wait_send()
        pair_copy(y, k, 1).wait_send()
        far_copy(k).wait_send()


def scatter_sum(part, slices):
    row_count, width = part.shape
    count = row_count // slices
    pieces = count // 16
    bf16 = jnp.bfloat16
    dma = pltpu.SemaphoreType.DMA
    return pl.pallas_call(
        functools.partial(sum_kernel, count),
        out_shape=jax.ShapeDtypeStruct((count, width), bf16),
        in_specs=[pl.BlockSpec(memory_space=pltpu.VMEM)],
        out_specs=pl.BlockSpec(memory_space=pltpu.VMEM),
        scratch_shapes=[
            pltpu.VMEM((2, count, width), bf16),
            pltpu.VMEM((count, width), bf16),
            pltpu.VMEM((count, width), bf16),
            dma((2, pieces)),
            dma((2, pieces)),
            dma((pieces,)),
            dma((pieces,)),
        ],
        compiler_params=pltpu.CompilerParams(
            collective_id=2, has_side_effects=True, vmem_limit_bytes=24 * 2**20
        ),
        cost_estimate=pl.CostEstimate(flops=0, bytes_accessed=2**25, transcendentals=0),
        name="scatter_sum",
    )(part)


def on_device(
    resid,
    pool_in,
    pool_mix,
    pool_gain,
    out_proj,
    norm_gain,
    w_gate,
    w_up,
    w_down,
    routes,
    route_weight,
):
    token_count, width = resid.shape
    choose = routes.shape[1]
    experts = lax.axis_size("sp")
    slices = lax.axis_size("tp")
    sub_count = token_count // slices
    capacity = max(2, 2 * sub_count * choose // experts)
    tp_index = lax.axis_index("tp")
    diff = group_diff(pool_in)
    pooled = (jnp.dot(diff, pool_mix[0], preferred_element_type=jnp.float32) * pool_gain).astype(
        jnp.bfloat16
    )
    group_part = rounded(jnp.dot(pooled, out_proj, preferred_element_type=jnp.float32)).astype(
        jnp.bfloat16
    )
    if slices == 4 and sub_count % 16 == 0:
        proj = scatter_sum(group_part, slices).astype(jnp.float32)
    else:
        proj = rounded(
            lax.psum_scatter(group_part, "tp", scatter_dimension=0, tiled=True).astype(jnp.float32)
        )
    first = tp_index * sub_count
    mixed = lax.dynamic_slice_in_dim(resid, first, sub_count, 0).astype(jnp.float32) + proj
    normed = normalize(mixed, norm_gain)
    route_rows = lax.dynamic_slice_in_dim(routes, first, sub_count, 0)
    weight_rows = lax.dynamic_slice_in_dim(route_weight, first, sub_count, 0)
    if experts == 8 and slices == 4 and sub_count == 2 * capacity and capacity % 16 == 0:
        table = token_table(route_rows, weight_rows, experts)
        moe = moe_exchange(normed, table, w_gate, w_up, w_down, capacity, experts)
    else:
        targets = slot_plan(route_rows, 1, capacity, experts)
        outgoing = fill_slots(normed, targets, experts * capacity)
        outgoing = outgoing.reshape(experts, capacity, width)
        arrived = lax.all_to_all(outgoing, "sp", split_axis=0, concat_axis=0, tiled=True)
        block_rows = lax.all_gather(arrived, "tp", axis=0, tiled=True)
        spread = expert_part(block_rows.reshape(-1, width), w_gate, w_up, w_down).reshape(
            block_rows.shape
        )
        stacked = spread.reshape((slices,) + arrived.shape)
        received = lax.all_to_all(stacked, "tp", split_axis=0, concat_axis=0, tiled=True)
        summed = jnp.sum(received.astype(jnp.float32), axis=0)
        returned = lax.all_to_all(
            summed.astype(jnp.bfloat16), "sp", split_axis=0, concat_axis=0, tiled=True
        )
        moe = collect(returned.reshape(-1, width), targets, weight_rows)
    return (mixed + moe).astype(jnp.bfloat16)


def solution(mesh):
    in_specs = (
        P("sp", None),
        P("sp", "tp"),
        P("tp", None, None),
        P("tp"),
        P("tp", None),
        P(),
        P("sp", None, "tp"),
        P("sp", None, "tp"),
        P("sp", "tp", None),
        P("sp", None),
        P("sp", None),
    )
    out_specs = P(("sp", "tp"), None)
    return jax.shard_map(
        on_device, mesh=mesh, in_specs=in_specs, out_specs=out_specs, check_vma=False
    )
```

```python
import functools

import jax
import jax.numpy as jnp
from jax import lax
from jax.experimental import pallas as pl
from jax.experimental.pallas import tpu as pltpu
from jax.sharding import PartitionSpec as P

GROUPS = 4


EPS = 1e-06


def shifted(x, axis, by):
    count = lax.axis_size(axis)
    pairs = [(i, i + by) for i in range(count) if 0 <= i + by < count]
    return lax.ppermute(x, axis, pairs)


def rounded(value):
    return lax.optimization_barrier(value.astype(jnp.bfloat16)).astype(jnp.float32)


def group_diff(pool_in):
    row_count = pool_in.shape[0]
    reach = 2**GROUPS
    before = shifted(pool_in[row_count - reach :], "sp", 1)
    joined = jnp.concatenate([before, pool_in], axis=0).astype(jnp.float32)
    running = jnp.cumsum(joined, axis=0)
    width = jnp.left_shift(jnp.int32(2), lax.axis_index("tp"))
    lagged = lax.dynamic_slice_in_dim(running, reach - width, row_count, 0)
    total = running[reach:] - lagged
    place = lax.axis_index("sp") * row_count + jnp.arange(row_count, dtype=jnp.int32) + 1
    counted = jnp.minimum(place, width).astype(jnp.float32)
    return (total / counted[:, None] - joined[reach:]).astype(jnp.bfloat16)


def normalize(mixed, norm_gain):
    scale = lax.rsqrt(jnp.mean(mixed * mixed, axis=1, keepdims=True) + EPS)
    return (mixed * scale * norm_gain).astype(jnp.bfloat16)


def slot_plan(route_rows, blocks, capacity, experts):
    row_count, choose = route_rows.shape
    flat_routes = route_rows.reshape(blocks, row_count // blocks * choose)
    onehot = (
        flat_routes[:, :, None] == jnp.arange(experts, dtype=jnp.int32)[None, None, :]
    ).astype(jnp.int32)
    earlier = jnp.cumsum(onehot, axis=1) - onehot
    position = jnp.sum(earlier * onehot, axis=2)
    block_ids = jnp.arange(blocks, dtype=jnp.int32)[:, None]
    return (flat_routes * (blocks * capacity) + block_ids * capacity + position).reshape(-1)


def fill_slots(normed, targets, slot_count):
    row_count, width = normed.shape
    slots = jnp.arange(slot_count, dtype=jnp.int32)[:, None, None]
    picks = jnp.sum((targets.reshape(row_count, -1)[None] == slots).astype(jnp.bfloat16), axis=2)
    return jnp.dot(picks, normed, preferred_element_type=jnp.float32).astype(normed.dtype)


def collect(returned, targets, weights):
    row_count, choose = weights.shape
    slots = jnp.arange(returned.shape[0], dtype=jnp.int32)[None, None, :]
    chosen = targets.reshape(row_count, choose)[:, :, None] == slots
    spread = jnp.sum(jnp.where(chosen, weights[:, :, None], 0.0), axis=1)
    head = lax.reduce_precision(spread, 8, 7)
    tail = spread - head
    both = jnp.concatenate([head, tail], axis=0).astype(jnp.bfloat16)
    product = jnp.dot(both, returned, preferred_element_type=jnp.float32)
    return product[:row_count] + product[row_count:]


def expert_part(inputs, w_gate, w_up, w_down):
    gate = jnp.dot(inputs, w_gate[0], preferred_element_type=jnp.float32)
    upper = jnp.dot(inputs, w_up[0], preferred_element_type=jnp.float32)
    hidden = (jax.nn.silu(gate) * upper).astype(jnp.bfloat16)
    return jnp.dot(hidden, w_down[0], preferred_element_type=jnp.float32).astype(jnp.bfloat16)


def line_plan(z):
    first = z + 1 - 2 * (z % 2)
    second = 2 - z // 2
    third = 3 - 3 * (z // 2)
    return first, second, third


def moe_kernel(
    front, back, capacity, experts,
    rows_in, meta_in, wg_hbm, wu_hbm, wd_hbm, out,
    wg, wu, wd, rows, meta, slots, give, parts,
    mate_in, y_in, x_in, sums, line_in, home_in, last_in, mixes,
    w_sem, m_send, m_recv, r_recv, ra_send, rb_send,
    xf_send, xf_recv, yf_send, yf_recv, mf_send, mf_recv,
    mb_send, mb_recv, yb_send, yb_recv, xb_send, xb_recv,
    zf_send, zf_recv, zh_send, zh_recv, yl_send, yl_recv,
):
    me = lax.axis_index("sp")
    tp = lax.axis_index("tp")
    z, x = me // 2, me % 2
    y, c = tp // 2, tp % 2
    C = capacity
    tokens, width = rows_in.shape
    wf, wb = width // front, width // back
    z1, z2, z3 = line_plan(z)
    mid = ((z + 1) // 2) % 2 == 1
    end = ((z + 1) // 2) % 2 == 0
    mate = (me, y * 2 + 1 - c)
    across = (me, (1 - y) * 2 + c)
    peer_expert = me + 1 - 2 * x
    beside = (peer_expert, tp)
    f32, bf16 = jnp.float32, jnp.bfloat16

    def plane(zz):
        return (zz * 2 + x, tp)

    def remote(src, dst, send, recv, to):
        return pltpu.make_async_remote_copy(
            src_ref=src, dst_ref=dst, send_sem=send, recv_sem=recv,
            device_id=to, device_id_type=pl.DeviceIdType.MESH,
        )

    def fcols(h):
        if h is None:
            return pl.ds(0, width)
        return pl.ds(pl.multiple_of(h * wf, wf), wf)

    def bcols(h):
        if h is None:
            return pl.ds(0, width)
        return pl.ds(pl.multiple_of(h * wb, wb), wb)

    def spot(xx, yy):
        return pl.ds(pl.multiple_of(c * 4 * C + xx * 2 * C + yy * C, C), C)

    def both(xx):
        return pl.ds(pl.multiple_of(c * 4 * C + xx * 2 * C, 2 * C), 2 * C)

    def half(cc):
        return pl.ds(pl.multiple_of(cc * 4 * C, 4 * C), 4 * C)

    def strip(yy):
        return pl.ds(pl.multiple_of(yy * C, C), C)

    def meta_copy(q):
        zq, yq = (z + q // 2) % 4, (y + q) % 2
        return remote(meta_in, meta.at[z, y], m_send.at[q], m_recv.at[z, y],
                      (zq * 2 + x, yq * 2 + c))

    def meta_here(zt, yt):
        remote(meta.at[zt, yt], meta.at[zt, yt], m_send.at[0], m_recv.at[zt, yt],
               mate).wait_recv()

    def at(h):
        return 0 if h is None else h

    def own_copy(h, to, send):
        return remote(rows_in.at[:, fcols(h)], rows.at[z, :, fcols(h)],
                      send.at[z], r_recv.at[z, at(h)], plane(to))

    def pass_copy(zt, h, to, send):
        ref = rows.at[zt, :, fcols(h)]
        return remote(ref, ref, send.at[zt], r_recv.at[zt, at(h)], plane(to))

    def xf_copy(zt, h):
        return remote(give.at[zt, :, fcols(h)], slots.at[zt, spot(x, y), fcols(h)],
                      xf_send.at[zt], xf_recv.at[zt, at(h)], beside)

    def yf_copy(zt, xx, h):
        ref = slots.at[zt, spot(xx, y), fcols(h)]
        return remote(ref, ref, yf_send.at[zt, xx], yf_recv.at[zt, xx, at(h)], across)

    def mf_copy(zt, h):
        ref = slots.at[zt, half(c), fcols(h)]
        return remote(ref, ref, mf_send.at[zt], mf_recv.at[zt, at(h)], mate)

    def mb_copy(zt, h):
        return remote(parts.at[zt, half(1 - c), bcols(h)], mate_in.at[zt, :, bcols(h)],
                      mb_send.at[zt], mb_recv.at[zt, at(h)], mate)

    def yb_copy(zt, xx, h):
        return remote(parts.at[zt, spot(xx, 1 - y), bcols(h)], y_in.at[zt, strip(xx), bcols(h)],
                      yb_send.at[zt, xx], yb_recv.at[zt, xx, at(h)], across)

    def xb_copy(zt, near, h):
        if near:
            return remote(parts.at[zt, both(1 - x), bcols(h)], x_in.at[zt, :, bcols(h)],
                          xb_send.at[zt], xb_recv.at[zt, at(h)], beside)
        return remote(parts.at[zt, spot(1 - x, y), bcols(h)], x_in.at[zt, strip(y), bcols(h)],
                      xb_send.at[zt], xb_recv.at[zt, at(h)], beside)

    def line_copy(zt, h, to):
        return remote(sums.at[zt, y, :, bcols(h)], line_in.at[zt, :, bcols(h)],
                      zf_send.at[zt], zf_recv.at[zt, at(h)], plane(to))

    def home_copy(zt, yt, side, h):
        return remote(sums.at[zt, yt, :, bcols(h)], home_in.at[side, yt, :, bcols(h)],
                      zh_send.at[side, yt], zh_recv.at[side, yt, at(h)], plane(zt))

    def home_here(yt, side, h):
        ref = home_in.at[side, yt, :, bcols(h)]
        remote(ref, ref, zh_send.at[side, yt], zh_recv.at[side, yt, at(h)], mate).wait_recv()

    def last_copy(h):
        return remote(sums.at[z, 1 - y, :, bcols(h)], last_in.at[:, bcols(h)],
                      yl_send, yl_recv.at[at(h)], across)

    loads = [
        pltpu.make_async_copy(wg_hbm.at[0], wg, w_sem.at[0]),
        pltpu.make_async_copy(wu_hbm.at[0], wu, w_sem.at[1]),
        pltpu.make_async_copy(wd_hbm.at[0], wd, w_sem.at[2]),
    ]

    barrier = pltpu.get_barrier_semaphore()
    for peer in (mate, beside):
        pl.semaphore_signal(barrier, inc=1, device_id=peer,
                            device_id_type=pl.DeviceIdType.MESH)

    @pl.loop(1, 8)
    def _(q):
        zq, yq = (z + q // 2) % 4, (y + q) % 2
        pl.semaphore_signal(barrier, inc=1, device_id=(zq * 2 + x, yq * 2 + c),
                            device_id_type=pl.DeviceIdType.MESH)

    pl.semaphore_wait(barrier, 9)

    @pl.loop(1, 8)
    def _(q):
        meta_copy(q).start()

    @pl.loop(0, front)
    def _(h):
        own_copy(h, z1, ra_send).start()

        @pl.when(mid)
        def _():
            own_copy(h, z2, rb_send).start()

    for load in loads:
        load.start()
    meta[z, y] = meta_in[...]
    rows[z] = rows_in[...]

    def picks_of(zt):
        places = meta[zt, y, :experts, :]
        level = lax.broadcasted_iota(jnp.int32, places.shape, 0)
        slot = lax.broadcasted_iota(jnp.int32, (C, tokens), 0).astype(f32)

        def one(expert):
            place = jnp.sum(jnp.where(level == expert, places, 0.0), axis=0, keepdims=True)
            return jnp.where(place[:, :tokens] == slot, 1.0, 0.0)

        return jnp.concatenate([one(me), one(peer_expert)], axis=0).astype(bf16)

    def gather(picks, zt, h):
        found = jnp.dot(picks, rows[zt, :, fcols(h)], preferred_element_type=f32)
        found = found.astype(bf16)
        give[zt, :, fcols(h)] = found[C:]
        xf_copy(zt, h).start()
        slots[zt, spot(x, y), fcols(h)] = found[:C]
        yf_copy(zt, x, h).start()

    def arrive(zt, onward):
        meta_here(zt, y)
        picks = picks_of(zt)

        @pl.loop(0, front)
        def _(h):
            pass_copy(zt, h, z1, ra_send).wait_recv()
            onward(h)
            gather(picks, zt, h)

    def nothing(h):
        pass

    def turn(zt):
        @pl.loop(0, front)
        def _(h):
            xf_copy(zt, h).wait_recv()
            yf_copy(zt, 1 - x, h).start()

    def complete(zt):
        @pl.loop(0, front)
        def _(h):
            yf_copy(zt, x, h).wait_recv()
            yf_copy(zt, 1 - x, h).wait_recv()
            mf_copy(zt, h).start()

    def compute(zt):
        @pl.loop(0, front)
        def _(h):
            mf_copy(zt, h).wait_recv()

        v = slots[zt]
        gate = jnp.dot(v, wg[...], preferred_element_type=f32)
        upper = jnp.dot(v, wu[...], preferred_element_type=f32)
        hidden = (gate * (1.0 / (1.0 + jnp.exp(-gate))) * upper).astype(bf16)

        @pl.loop(0, back)
        def _(h):
            parts[zt, :, bcols(h)] = jnp.dot(
                hidden, wd[:, bcols(h)], preferred_element_type=f32
            ).astype(bf16)
            mb_copy(zt, h).start()

    def pair_sum(zt, far, first=0, stop=back):
        @pl.loop(first, stop)
        def _(h):
            mb_copy(zt, h).wait_recv()
            total = (
                parts[zt, half(c), bcols(h)].astype(f32) + mate_in[zt, :, bcols(h)].astype(f32)
            )
            parts[zt, half(c), bcols(h)] = total.astype(bf16)
            if far:
                yb_copy(zt, 0, h).start()
                yb_copy(zt, 1, h).start()
            else:
                xb_copy(zt, True, h).start()

    def far_piece(zt, h):
        for xx in (0, 1):
            yb_copy(zt, xx, h).wait_recv()
            total = (
                parts[zt, spot(xx, y), bcols(h)].astype(f32)
                + y_in[zt, strip(xx), bcols(h)].astype(f32)
            )
            parts[zt, spot(xx, y), bcols(h)] = total.astype(bf16)
        xb_copy(zt, False, h).start()

    def far_sum(zt):
        @pl.loop(0, back)
        def _(h):
            far_piece(zt, h)

    def weights_of(zt, yt):
        places = meta[zt, yt, :experts, :]
        shares = meta[zt, yt, experts:, :]
        level = lax.broadcasted_iota(jnp.int32, places.shape, 0)
        slot = lax.broadcasted_iota(jnp.int32, (C, places.shape[1]), 0).astype(f32)

        def one(expert):
            place = jnp.sum(jnp.where(level == expert, places, 0.0), axis=0, keepdims=True)
            share = jnp.sum(jnp.where(level == expert, shares, 0.0), axis=0, keepdims=True)
            spread = jnp.where(place == slot, share, 0.0)
            head = spread.astype(bf16).astype(f32)
            return head, spread - head

        mine, theirs = one(me), one(peer_expert)
        both = jnp.concatenate([mine[0], theirs[0], mine[1], theirs[1]], axis=0)
        return both.T[:tokens].astype(bf16)

    def blend(spread, zt, yt, h):
        mine = parts[zt, spot(x, yt), bcols(h)]
        theirs = x_in[zt, strip(yt), bcols(h)]
        pair = jnp.concatenate([mine, theirs, mine, theirs], axis=0)
        return jnp.dot(spread, pair, preferred_element_type=f32)

    def near_other(zt, side, first=0, stop=back):
        there = weights_of(zt, 1 - y)

        @pl.loop(first, stop)
        def _(h):
            xb_copy(zt, True, h).wait_recv()
            sums[zt, 1 - y, :, bcols(h)] = blend(there, zt, 1 - y, h).astype(bf16)
            home_copy(zt, 1 - y, side, h).start()

    def near_same(zt, side, first=0, stop=back):
        here = weights_of(zt, y)

        @pl.loop(first, stop)
        def _(h):
            total = blend(here, zt, y, h)

            @pl.when(mid)
            def _():
                line_copy(zt, h, z1).wait_recv()
                sums[zt, y, :, bcols(h)] = (
                    total + line_in[zt, :, bcols(h)].astype(f32)
                ).astype(bf16)

            @pl.when(end)
            def _():
                sums[zt, y, :, bcols(h)] = total.astype(bf16)

            home_copy(zt, y, side, h).start()

    def far_back():
        mixes[0] = weights_of(z3, y)
        mixes[1] = weights_of(z1, y)

        @pl.loop(0, back + LAG)
        def _(i):
            @pl.when(i < back)
            def _():
                xb_copy(z3, False, i).wait_recv()
                total = blend(mixes[0], z3, y, i)
                line_copy(z3, i, z1).wait_recv()
                sums[z3, y, :, bcols(i)] = (
                    total + line_in[z3, :, bcols(i)].astype(f32)
                ).astype(bf16)
                line_copy(z3, i, z2).start()

            @pl.when(i >= LAG)
            def _():
                k = i - LAG
                total = blend(mixes[1], z1, y, k)
                line_copy(z1, k, z1).wait_recv()
                sums[z1, y, :, bcols(k)] = (
                    total + line_in[z1, :, bcols(k)].astype(f32)
                ).astype(bf16)
                home_copy(z1, y, 0, k).start()

    def far_chain():
        mixes[0] = weights_of(z2, y)
        mixes[1] = weights_of(z3, y)

        @pl.loop(0, 2 * back + LAG)
        def _(i):
            @pl.when(i < 2 * back)
            def _():
                far_piece(z2 + (z3 - z2) * (i // back), i % back)

            @pl.when(i >= LAG)
            def _():
                k = i - LAG
                which, h = k // back, k % back
                zt = z2 + (z3 - z2) * which
                xb_copy(zt, False, h).wait_recv()
                sums[zt, y, :, bcols(h)] = blend(mixes[which], zt, y, h).astype(bf16)
                line_copy(zt, h, z1).start()

    def own_back():
        here = weights_of(z, y)
        there = weights_of(z, 1 - y)

        @pl.loop(0, back)
        def _(h):
            xb_copy(z, True, h).wait_recv()
            sums[z, 1 - y, :, bcols(h)] = blend(there, z, 1 - y, h).astype(bf16)
            out[:, bcols(h)] = blend(here, z, y, h)

    def last_send():
        @pl.loop(0, back)
        def _(h):
            home_here(1 - y, 0, h)
            total = (
                sums[z, 1 - y, :, bcols(h)].astype(f32) + home_in[0, 1 - y, :, bcols(h)].astype(f32)
            )

            @pl.when(mid)
            def _():
                home_here(1 - y, 1, h)
                sums[z, 1 - y, :, bcols(h)] = (
                    total + home_in[1, 1 - y, :, bcols(h)].astype(f32)
                ).astype(bf16)

            @pl.when(end)
            def _():
                sums[z, 1 - y, :, bcols(h)] = total.astype(bf16)

            last_copy(h).start()

    def finish():
        @pl.loop(0, back)
        def _(h):
            home_here(y, 0, h)
            total = out[:, bcols(h)] + home_in[0, y, :, bcols(h)].astype(f32)

            @pl.when(mid)
            def _():
                home_here(y, 1, h)
                out[:, bcols(h)] = total + home_in[1, y, :, bcols(h)].astype(f32)

            @pl.when(end)
            def _():
                out[:, bcols(h)] = total

            last_copy(h).wait_recv()
            out[:, bcols(h)] += last_in[:, bcols(h)].astype(f32)

    def scoped(fn, name):
        def run(*args):
            with jax.named_scope(name):
                fn(*args)
        return run

    arrive = scoped(arrive, "arrive")
    turn = scoped(turn, "turn")
    complete = scoped(complete, "complete")
    compute = scoped(compute, "compute")
    pair_sum = scoped(pair_sum, "pair_sum")
    far_sum = scoped(far_sum, "far_sum")
    near_other = scoped(near_other, "near_other")
    near_same = scoped(near_same, "near_same")
    far_back = scoped(far_back, "far_back")
    own_back = scoped(own_back, "own_back")
    last_send = scoped(last_send, "last_send")
    far_chain = scoped(far_chain, "far_chain")

    def onto(zt, to, send):
        return lambda h: pass_copy(zt, h, to, send).start()

    def first_on(h):
        @pl.when(mid)
        def _():
            pass_copy(z1, h, z2, rb_send).start()

    meta_picks = picks_of(z)

    @pl.loop(0, front)
    def _(h):
        gather(meta_picks, z, h)

    turn(z)
    arrive(z1, first_on)

    @pl.when(mid)
    def _():
        arrive(z2, onto(z2, z1, ra_send))

    turn(z1)

    @pl.when(mid)
    def _():
        turn(z2)
        arrive(z3, onto(z3, z1, ra_send))

    complete(z)
    for zt in (z, z1, z2, z3):
        meta_here(zt, 1 - y)
    for load in loads:
        load.wait()
    compute(z)

    @pl.when(end)
    def _():
        arrive(z2, nothing)

    complete(z1)
    compute(z1)

    @pl.when(end)
    def _():
        turn(z2)
        pair_sum(z1, False, 0, back // 2)
        arrive(z3, nothing)
        pair_sum(z1, False, back // 2, back)
        near_other(z1, 0, 0, back // 2)

    @pl.when(mid)
    def _():
        turn(z3)
        pair_sum(z1, False)

    complete(z2)
    compute(z2)

    @pl.when(end)
    def _():
        turn(z3)
        pair_sum(z2, True)
        near_other(z1, 0, back // 2, back)
        near_same(z1, 0)
        pair_sum(z, False)

    @pl.when(mid)
    def _():
        pair_sum(z2, False)

    complete(z3)
    compute(z3)
    pair_sum(z3, True)

    @pl.when(end)
    def _():
        far_chain()
        own_back()
        last_send()

    @pl.when(mid)
    def _():
        pair_sum(z, False)
        near_other(z1, 0)
        near_other(z2, 1)
        far_sum(z3)
        own_back()
        last_send()
        near_same(z2, 1)
        far_back()

    with jax.named_scope("finish"):
        finish()

    @pl.loop(1, 8)
    def _(q):
        meta_copy(q).wait_send()

    own_copy(None, z1, ra_send).wait_send()
    for zt in (z, z1, z2, z3):
        xf_copy(zt, None).wait_send()
        yf_copy(zt, 0, None).wait_send()
        yf_copy(zt, 1, None).wait_send()
        mf_copy(zt, None).wait_send()
        mb_copy(zt, None).wait_send()
    xb_copy(z, True, None).wait_send()
    xb_copy(z1, True, None).wait_send()
    xb_copy(z3, False, None).wait_send()
    yb_copy(z3, 0, None).wait_send()
    yb_copy(z3, 1, None).wait_send()
    line_copy(z3, None, z1).wait_send()
    home_copy(z1, 0, 0, None).wait_send()
    home_copy(z1, 1, 0, None).wait_send()
    last_copy(None).wait_send()

    @pl.when(mid)
    def _():
        own_copy(None, z2, rb_send).wait_send()
        pass_copy(z1, None, z2, rb_send).wait_send()
        pass_copy(z2, None, z1, ra_send).wait_send()
        pass_copy(z3, None, z1, ra_send).wait_send()
        xb_copy(z2, True, None).wait_send()
        home_copy(z2, 0, 1, None).wait_send()
        home_copy(z2, 1, 1, None).wait_send()

    @pl.when(end)
    def _():
        xb_copy(z2, False, None).wait_send()
        yb_copy(z2, 0, None).wait_send()
        yb_copy(z2, 1, None).wait_send()
        line_copy(z2, None, z1).wait_send()


FRONT, BACK, LAG = 4, 4, 2


def moe_exchange(normed, meta, w_gate, w_up, w_down, capacity, experts):
    tokens, width = normed.shape
    units = w_gate.shape[2]
    bf16 = jnp.bfloat16
    dma = pltpu.SemaphoreType.DMA
    C = capacity
    vmem = pltpu.VMEM

    def lanes(*shape, pieces):
        return [dma(shape), dma(shape + (pieces,))]

    return pl.pallas_call(
        functools.partial(moe_kernel, FRONT, BACK, capacity, experts),
        out_shape=jax.ShapeDtypeStruct((tokens, width), jnp.float32),
        in_specs=[pl.BlockSpec(memory_space=pltpu.VMEM)] * 2
        + [pl.BlockSpec(memory_space=pl.ANY)] * 3,
        out_specs=pl.BlockSpec(memory_space=pltpu.VMEM),
        scratch_shapes=[
            vmem((width, units), bf16),
            vmem((width, units), bf16),
            vmem((units, width), bf16),
            vmem((4, tokens, width), bf16),
            vmem((4, 2) + meta.shape, jnp.float32),
            vmem((4, 8 * C, width), bf16),
            vmem((4, C, width), bf16),
            vmem((4, 8 * C, width), bf16),
            vmem((4, 4 * C, width), bf16),
            vmem((4, 2 * C, width), bf16),
            vmem((4, 2 * C, width), bf16),
            vmem((4, 2, tokens, width), bf16),
            vmem((4, tokens, width), bf16),
            vmem((2, 2, tokens, width), bf16),
            vmem((tokens, width), bf16),
            vmem((2, tokens, 4 * C), bf16),
            dma((3,)), dma((8,)), dma((4, 2)), dma((4, FRONT)), dma((4,)), dma((4,)),
        ]
        + lanes(4, pieces=FRONT) + lanes(4, 2, pieces=FRONT) + lanes(4, pieces=FRONT)
        + lanes(4, pieces=BACK) + lanes(4, 2, pieces=BACK) + lanes(4, pieces=BACK)
        + lanes(4, pieces=BACK) + lanes(2, 2, pieces=BACK) + [dma, dma((BACK,))],
        compiler_params=pltpu.CompilerParams(
            collective_id=1, has_side_effects=True, vmem_limit_bytes=60 * 2**20
        ),
        cost_estimate=pl.CostEstimate(
            flops=6 * experts * 4 * C * width * units,
            bytes_accessed=3 * 2 * width * units,
            transcendentals=0,
        ),
        name="moe_exchange",
    )(normed, meta, w_gate, w_up, w_down)


def token_table(route_rows, weight_rows, experts):
    row_count = route_rows.shape[0]
    f32 = jnp.float32
    chosen = route_rows[:, :, None] == jnp.arange(experts, dtype=jnp.int32)[None, None, :]
    hit = jnp.any(chosen, axis=1)
    order = jnp.arange(row_count)
    earlier = (order[:, None] > order[None, :]).astype(jnp.bfloat16)
    place = jnp.dot(earlier, hit.astype(jnp.bfloat16), preferred_element_type=f32)
    place = jnp.where(hit, place, -1.0)
    weight = jnp.sum(jnp.where(chosen, weight_rows[:, :, None], 0.0), axis=1)
    both = jnp.concatenate([place.T, weight.T], axis=0)
    return jnp.pad(both, ((0, 0), (0, 128 - row_count)), constant_values=-1.0)


def sum_kernel(count, part, out, pair_in, total, y_in, pp_send, pp_recv, y_send, y_recv):
    me = lax.axis_index("sp")
    tp = lax.axis_index("tp")
    core, y = tp % 2, tp // 2
    mate = y * 2 + (1 - core)
    across = (1 - y) * 2 + core
    pieces = count // 16
    mesh_id = pl.DeviceIdType.MESH
    barrier = pltpu.get_barrier_semaphore()
    for peer in (mate, across):
        pl.semaphore_signal(barrier, inc=1, device_id=(me, peer), device_id_type=mesh_id)
    pl.semaphore_wait(barrier, 2)

    def at(yy, c, k):
        return pl.ds(pl.multiple_of((yy * 2 + c) * count + k * 16, 16), 16)

    def piece(k):
        return pl.ds(pl.multiple_of(k * 16, 16), 16)

    def pair_copy(yy, k, place):
        return pltpu.make_async_remote_copy(
            src_ref=part.at[at(yy, 1 - core, k)], dst_ref=pair_in.at[place, piece(k)],
            send_sem=pp_send.at[place, k], recv_sem=pp_recv.at[place, k],
            device_id=(me, mate), device_id_type=mesh_id,
        )

    def far_copy(k):
        return pltpu.make_async_remote_copy(
            src_ref=total.at[piece(k)], dst_ref=y_in.at[piece(k)],
            send_sem=y_send.at[k], recv_sem=y_recv.at[k],
            device_id=(me, across), device_id_type=mesh_id,
        )

    @pl.loop(0, pieces)
    def _(k):
        pair_copy(1 - y, k, 0).start()

    @pl.loop(0, pieces)
    def _(k):
        pair_copy(y, k, 1).start()

    @pl.loop(0, pieces)
    def _(k):
        pair_copy(1 - y, k, 0).wait_recv()
        total[piece(k)] = (
            part[at(1 - y, core, k)].astype(jnp.float32)
            + pair_in[0, piece(k)].astype(jnp.float32)
        ).astype(jnp.bfloat16)
        far_copy(k).start()

    @pl.loop(0, pieces)
    def _(k):
        pair_copy(y, k, 1).wait_recv()
        far_copy(k).wait_recv()
        out[piece(k)] = (
            part[at(y, core, k)].astype(jnp.float32)
            + pair_in[1, piece(k)].astype(jnp.float32)
            + y_in[piece(k)].astype(jnp.float32)
        ).astype(jnp.bfloat16)

    @pl.loop(0, pieces)
    def _(k):
        pair_copy(1 - y, k, 0).wait_send()
        pair_copy(y, k, 1).wait_send()
        far_copy(k).wait_send()


def scatter_sum(part, slices):
    row_count, width = part.shape
    count = row_count // slices
    pieces = count // 16
    bf16 = jnp.bfloat16
    dma = pltpu.SemaphoreType.DMA
    return pl.pallas_call(
        functools.partial(sum_kernel, count),
        out_shape=jax.ShapeDtypeStruct((count, width), bf16),
        in_specs=[pl.BlockSpec(memory_space=pltpu.VMEM)],
        out_specs=pl.BlockSpec(memory_space=pltpu.VMEM),
        scratch_shapes=[
            pltpu.VMEM((2, count, width), bf16),
            pltpu.VMEM((count, width), bf16),
            pltpu.VMEM((count, width), bf16),
            dma((2, pieces)),
            dma((2, pieces)),
            dma((pieces,)),
            dma((pieces,)),
        ],
        compiler_params=pltpu.CompilerParams(
            collective_id=2, has_side_effects=True, vmem_limit_bytes=24 * 2**20
        ),
        cost_estimate=pl.CostEstimate(flops=0, bytes_accessed=2**25, transcendentals=0),
        name="scatter_sum",
    )(part)


def on_device(
    resid,
    pool_in,
    pool_mix,
    pool_gain,
    out_proj,
    norm_gain,
    w_gate,
    w_up,
    w_down,
    routes,
    route_weight,
):
    token_count, width = resid.shape
    choose = routes.shape[1]
    experts = lax.axis_size("sp")
    slices = lax.axis_size("tp")
    sub_count = token_count // slices
    capacity = max(2, 2 * sub_count * choose // experts)
    tp_index = lax.axis_index("tp")
    diff = group_diff(pool_in)
    pooled = (jnp.dot(diff, pool_mix[0], preferred_element_type=jnp.float32) * pool_gain).astype(
        jnp.bfloat16
    )
    group_part = rounded(jnp.dot(pooled, out_proj, preferred_element_type=jnp.float32)).astype(
        jnp.bfloat16
    )
    if slices == 4 and sub_count % 16 == 0:
        proj = scatter_sum(group_part, slices).astype(jnp.float32)
    else:
        proj = rounded(
            lax.psum_scatter(group_part, "tp", scatter_dimension=0, tiled=True).astype(jnp.float32)
        )
    first = tp_index * sub_count
    mixed = lax.dynamic_slice_in_dim(resid, first, sub_count, 0).astype(jnp.float32) + proj
    normed = normalize(mixed, norm_gain)
    route_rows = lax.dynamic_slice_in_dim(routes, first, sub_count, 0)
    weight_rows = lax.dynamic_slice_in_dim(route_weight, first, sub_count, 0)
    if experts == 8 and slices == 4 and sub_count == 2 * capacity and capacity % 16 == 0:
        table = token_table(route_rows, weight_rows, experts)
        moe = moe_exchange(normed, table, w_gate, w_up, w_down, capacity, experts)
    else:
        targets = slot_plan(route_rows, 1, capacity, experts)
        outgoing = fill_slots(normed, targets, experts * capacity)
        outgoing = outgoing.reshape(experts, capacity, width)
        arrived = lax.all_to_all(outgoing, "sp", split_axis=0, concat_axis=0, tiled=True)
        block_rows = lax.all_gather(arrived, "tp", axis=0, tiled=True)
        spread = expert_part(block_rows.reshape(-1, width), w_gate, w_up, w_down).reshape(
            block_rows.shape
        )
        stacked = spread.reshape((slices,) + arrived.shape)
        received = lax.all_to_all(stacked, "tp", split_axis=0, concat_axis=0, tiled=True)
        summed = jnp.sum(received.astype(jnp.float32), axis=0)
        returned = lax.all_to_all(
            summed.astype(jnp.bfloat16), "sp", split_axis=0, concat_axis=0, tiled=True
        )
        moe = collect(returned.reshape(-1, width), targets, weight_rows)
    return (mixed + moe).astype(jnp.bfloat16)


def solution(mesh):
    in_specs = (
        P("sp", None),
        P("sp", "tp"),
        P("tp", None, None),
        P("tp"),
        P("tp", None),
        P(),
        P("sp", None, "tp"),
        P("sp", None, "tp"),
        P("sp", "tp", None),
        P("sp", None),
        P("sp", None),
    )
    out_specs = P(("sp", "tp"), None)
    return jax.shard_map(
        on_device, mesh=mesh, in_specs=in_specs, out_specs=out_specs, check_vma=False
    )
```

```python
import functools

import jax
import jax.numpy as jnp
from jax import lax
from jax.experimental import pallas as pl
from jax.experimental.pallas import tpu as pltpu
from jax.sharding import PartitionSpec as P

GROUPS = 4


EPS = 1e-06


def shifted(x, axis, by):
    count = lax.axis_size(axis)
    pairs = [(i, i + by) for i in range(count) if 0 <= i + by < count]
    return lax.ppermute(x, axis, pairs)


def rounded(value):
    return lax.optimization_barrier(value.astype(jnp.bfloat16)).astype(jnp.float32)


def group_diff(pool_in):
    row_count = pool_in.shape[0]
    reach = 2**GROUPS
    before = shifted(pool_in[row_count - reach :], "sp", 1)
    joined = jnp.concatenate([before, pool_in], axis=0).astype(jnp.float32)
    running = jnp.cumsum(joined, axis=0)
    width = jnp.left_shift(jnp.int32(2), lax.axis_index("tp"))
    lagged = lax.dynamic_slice_in_dim(running, reach - width, row_count, 0)
    total = running[reach:] - lagged
    place = lax.axis_index("sp") * row_count + jnp.arange(row_count, dtype=jnp.int32) + 1
    counted = jnp.minimum(place, width).astype(jnp.float32)
    return (total / counted[:, None] - joined[reach:]).astype(jnp.bfloat16)


def normalize(mixed, norm_gain):
    scale = lax.rsqrt(jnp.mean(mixed * mixed, axis=1, keepdims=True) + EPS)
    return (mixed * scale * norm_gain).astype(jnp.bfloat16)


def slot_plan(route_rows, blocks, capacity, experts):
    row_count, choose = route_rows.shape
    flat_routes = route_rows.reshape(blocks, row_count // blocks * choose)
    onehot = (
        flat_routes[:, :, None] == jnp.arange(experts, dtype=jnp.int32)[None, None, :]
    ).astype(jnp.int32)
    earlier = jnp.cumsum(onehot, axis=1) - onehot
    position = jnp.sum(earlier * onehot, axis=2)
    block_ids = jnp.arange(blocks, dtype=jnp.int32)[:, None]
    return (flat_routes * (blocks * capacity) + block_ids * capacity + position).reshape(-1)


def fill_slots(normed, targets, slot_count):
    row_count, width = normed.shape
    slots = jnp.arange(slot_count, dtype=jnp.int32)[:, None, None]
    picks = jnp.sum((targets.reshape(row_count, -1)[None] == slots).astype(jnp.bfloat16), axis=2)
    return jnp.dot(picks, normed, preferred_element_type=jnp.float32).astype(normed.dtype)


def collect(returned, targets, weights):
    row_count, choose = weights.shape
    slots = jnp.arange(returned.shape[0], dtype=jnp.int32)[None, None, :]
    chosen = targets.reshape(row_count, choose)[:, :, None] == slots
    spread = jnp.sum(jnp.where(chosen, weights[:, :, None], 0.0), axis=1)
    head = lax.reduce_precision(spread, 8, 7)
    tail = spread - head
    both = jnp.concatenate([head, tail], axis=0).astype(jnp.bfloat16)
    product = jnp.dot(both, returned, preferred_element_type=jnp.float32)
    return product[:row_count] + product[row_count:]


def expert_part(inputs, w_gate, w_up, w_down):
    gate = jnp.dot(inputs, w_gate[0], preferred_element_type=jnp.float32)
    upper = jnp.dot(inputs, w_up[0], preferred_element_type=jnp.float32)
    hidden = (jax.nn.silu(gate) * upper).astype(jnp.bfloat16)
    return jnp.dot(hidden, w_down[0], preferred_element_type=jnp.float32).astype(jnp.bfloat16)


def line_plan(z):
    first = z + 1 - 2 * (z % 2)
    second = 2 - z // 2
    third = 3 - 3 * (z // 2)
    return first, second, third


def moe_kernel(
    front, back, capacity, experts,
    resid, pool_in, pool_mix, pool_gain, out_proj, norm_gain,
    wg_hbm, wu_hbm, wd_hbm, routes, shares_in, out,
    pool, mix, gain, proj, scales, named, shares, stay, halo, pooled, part,
    pair_in, far_out, far_in, mixed, meta_in,
    wg, wu, wd, rows, meta, slots, give, parts,
    mate_in, y_in, x_in, sums, line_in, home_in, last_in, mixes,
    w_sem, h_send, h_recv, pp_send, pp_recv, fy_send, fy_recv,
    m_send, m_recv, r_recv, ra_send, rb_send,
    xf_send, xf_recv, yf_send, yf_recv, mf_send, mf_recv,
    mb_send, mb_recv, yb_send, yb_recv, xb_send, xb_recv,
    zf_send, zf_recv, zh_send, zh_recv, yl_send, yl_recv,
):
    me = lax.axis_index("sp")
    tp = lax.axis_index("tp")
    z, x = me // 2, me % 2
    y, c = tp // 2, tp % 2
    C = capacity
    tokens, width = out.shape
    count = lax.axis_size("sp")
    row_count = pool.shape[0]
    reach = halo.shape[0]
    first = pl.multiple_of(tp * tokens, tokens)
    pieces = tokens // 16
    wf, wb = width // front, width // back
    z1, z2, z3 = line_plan(z)
    mid = ((z + 1) // 2) % 2 == 1
    end = ((z + 1) // 2) % 2 == 0
    mate = (me, y * 2 + 1 - c)
    across = (me, (1 - y) * 2 + c)
    peer_expert = me + 1 - 2 * x
    beside = (peer_expert, tp)
    f32, bf16 = jnp.float32, jnp.bfloat16

    def plane(zz):
        return (zz * 2 + x, tp)

    def remote(src, dst, send, recv, to):
        return pltpu.make_async_remote_copy(
            src_ref=src, dst_ref=dst, send_sem=send, recv_sem=recv,
            device_id=to, device_id_type=pl.DeviceIdType.MESH,
        )

    def fcols(h):
        if h is None:
            return pl.ds(0, width)
        return pl.ds(pl.multiple_of(h * wf, wf), wf)

    def bcols(h):
        if h is None:
            return pl.ds(0, width)
        return pl.ds(pl.multiple_of(h * wb, wb), wb)

    def spot(xx, yy):
        return pl.ds(pl.multiple_of(c * 4 * C + xx * 2 * C + yy * C, C), C)

    def both(xx):
        return pl.ds(pl.multiple_of(c * 4 * C + xx * 2 * C, 2 * C), 2 * C)

    def half(cc):
        return pl.ds(pl.multiple_of(cc * 4 * C, 4 * C), 4 * C)

    def strip(yy):
        return pl.ds(pl.multiple_of(yy * C, C), C)

    def meta_copy(q):
        zq, yq = (z + q // 2) % 4, (y + q) % 2
        return remote(meta_in, meta.at[z, y], m_send.at[q], m_recv.at[z, y],
                      (zq * 2 + x, yq * 2 + c))

    def meta_here(zt, yt):
        remote(meta.at[zt, yt], meta.at[zt, yt], m_send.at[0], m_recv.at[zt, yt],
               mate).wait_recv()

    def at(h):
        return 0 if h is None else h

    def piece(k):
        if k is None:
            return pl.ds(0, tokens)
        return pl.ds(pl.multiple_of(k * 16, 16), 16)

    def block(yy, cc):
        return pl.multiple_of((yy * 2 + cc) * tokens, tokens)

    def block_piece(yy, cc, k):
        return pl.ds(pl.multiple_of(block(yy, cc) + k * 16, 16), 16)

    def halo_copy():
        return remote(pool.at[pl.ds(row_count - reach, reach)], halo, h_send, h_recv,
                      (me + 1, tp))

    def pair_copy(yy, place, k):
        if k is None:
            return remote(part.at[pl.ds(block(yy, 1 - c), tokens)], pair_in.at[place],
                          pp_send.at[place], pp_recv.at[place, 0], mate)
        return remote(part.at[block_piece(yy, 1 - c, k)], pair_in.at[place, piece(k)],
                      pp_send.at[place], pp_recv.at[place, k], mate)

    def far_copy(k):
        return remote(far_out.at[piece(k)], far_in.at[piece(k)],
                      fy_send, fy_recv.at[at(k)], across)

    def pass_copy(zt, h, to, send):
        ref = rows.at[zt, piece(h)]
        return remote(ref, ref, send.at[zt], r_recv.at[zt, at(h)], plane(to))

    def xf_copy(zt, h):
        return remote(give.at[zt, :, fcols(h)], slots.at[zt, spot(x, y), fcols(h)],
                      xf_send.at[zt], xf_recv.at[zt, at(h)], beside)

    def yf_copy(zt, xx, h):
        ref = slots.at[zt, spot(xx, y), fcols(h)]
        return remote(ref, ref, yf_send.at[zt, xx], yf_recv.at[zt, xx, at(h)], across)

    def mf_copy(zt, h):
        ref = slots.at[zt, half(c), fcols(h)]
        return remote(ref, ref, mf_send.at[zt], mf_recv.at[zt, at(h)], mate)

    def mb_copy(zt, h):
        return remote(parts.at[zt, half(1 - c), bcols(h)], mate_in.at[zt, :, bcols(h)],
                      mb_send.at[zt], mb_recv.at[zt, at(h)], mate)

    def yb_copy(zt, xx, h):
        return remote(parts.at[zt, spot(xx, 1 - y), bcols(h)], y_in.at[zt, strip(xx), bcols(h)],
                      yb_send.at[zt, xx], yb_recv.at[zt, xx, at(h)], across)

    def xb_copy(zt, near, h):
        if near:
            return remote(parts.at[zt, both(1 - x), bcols(h)], x_in.at[zt, :, bcols(h)],
                          xb_send.at[zt], xb_recv.at[zt, at(h)], beside)
        return remote(parts.at[zt, spot(1 - x, y), bcols(h)], x_in.at[zt, strip(y), bcols(h)],
                      xb_send.at[zt], xb_recv.at[zt, at(h)], beside)

    def line_copy(zt, h, to):
        return remote(sums.at[zt, y, :, bcols(h)], line_in.at[zt, :, bcols(h)],
                      zf_send.at[zt], zf_recv.at[zt, at(h)], plane(to))

    def home_copy(zt, yt, side, h):
        return remote(sums.at[zt, yt, :, bcols(h)], home_in.at[side, yt, :, bcols(h)],
                      zh_send.at[side, yt], zh_recv.at[side, yt, at(h)], plane(zt))

    def home_here(yt, side, h):
        ref = home_in.at[side, yt, :, bcols(h)]
        remote(ref, ref, zh_send.at[side, yt], zh_recv.at[side, yt, at(h)], mate).wait_recv()

    def last_copy(h):
        return remote(sums.at[z, 1 - y, :, bcols(h)], last_in.at[:, bcols(h)],
                      yl_send, yl_recv.at[at(h)], across)

    small = [
        pltpu.make_async_copy(pool_in, pool, w_sem.at[3]),
        pltpu.make_async_copy(routes, named, w_sem.at[4]),
        pltpu.make_async_copy(shares_in, shares, w_sem.at[5]),
        pltpu.make_async_copy(pool_mix.at[0], mix, w_sem.at[6]),
        pltpu.make_async_copy(pool_gain, gain, w_sem.at[7]),
        pltpu.make_async_copy(out_proj, proj, w_sem.at[8]),
        pltpu.make_async_copy(resid.at[pl.ds(first, tokens)], stay, w_sem.at[9]),
        pltpu.make_async_copy(norm_gain, scales, w_sem.at[10]),
    ]
    loads = [
        pltpu.make_async_copy(wg_hbm.at[0], wg, w_sem.at[0]),
        pltpu.make_async_copy(wu_hbm.at[0], wu, w_sem.at[1]),
        pltpu.make_async_copy(wd_hbm.at[0], wd, w_sem.at[2]),
    ]
    for load in small + loads:
        load.start()

    barrier = pltpu.get_barrier_semaphore()
    for peer in (mate, beside):
        pl.semaphore_signal(barrier, inc=1, device_id=peer,
                            device_id_type=pl.DeviceIdType.MESH)

    @pl.when(me > 0)
    def _():
        pl.semaphore_signal(barrier, inc=1, device_id=(me - 1, tp),
                            device_id_type=pl.DeviceIdType.MESH)

    @pl.loop(1, 8)
    def _(q):
        zq, yq = (z + q // 2) % 4, (y + q) % 2
        pl.semaphore_signal(barrier, inc=1, device_id=(zq * 2 + x, yq * 2 + c),
                            device_id_type=pl.DeviceIdType.MESH)

    pl.semaphore_wait(barrier, 9 + (2 * count - 2 - me) // count)
    small[0].wait()

    @pl.when(me < count - 1)
    def _():
        halo_copy().start()

    for load in small[1:]:
        load.wait()

    level = lax.broadcasted_iota(jnp.int32, (experts, row_count), 0)
    one_is, two_is = named[0:1, :] == level, named[1:2, :] == level
    hit = jnp.where(one_is | two_is, 1.0, 0.0)
    share = jnp.where(one_is, shares[0:1, :], 0.0) + jnp.where(two_is, shares[1:2, :], 0.0)
    head = share.astype(bf16).astype(f32)
    stack = jnp.concatenate([hit, head, share - head, hit], axis=0).astype(bf16)
    row = lax.broadcasted_iota(jnp.int32, (row_count, 128), 0)
    lane = lax.broadcasted_iota(jnp.int32, (row_count, 128), 1)
    inside = lane < tokens
    here = jnp.where((row == lane + first) & inside, 1.0, 0.0).astype(bf16)
    ahead = jnp.where((row >= first) & (row < lane + first) & inside, 1.0, 0.0).astype(bf16)
    taken = jnp.dot(stack, here, preferred_element_type=f32)
    before = jnp.dot(stack, ahead, preferred_element_type=f32)
    table = jnp.concatenate(
        [
            jnp.where(taken[:experts] > 0.5, before[:experts], -1.0),
            taken[experts:2 * experts] + taken[2 * experts:3 * experts],
        ],
        axis=0,
    )
    meta_in[...] = table
    meta[z, y] = table

    @pl.when(me == 0)
    def _():
        halo[...] = jnp.zeros(halo.shape, bf16)

    @pl.when(me > 0)
    def _():
        halo_copy().wait_recv()

    joined = jnp.concatenate([halo[...], pool[...]], axis=0).astype(f32)
    runs = [joined]
    for by in (1, 2, 4, 8):
        runs.append(runs[-1] + pltpu.roll(runs[-1], by, 0))
    total = jnp.where(
        tp == 0, runs[1], jnp.where(tp == 1, runs[2], jnp.where(tp == 2, runs[3], runs[4]))
    )[reach:]
    span = jnp.where(tp == 0, 2, jnp.where(tp == 1, 4, jnp.where(tp == 2, 8, 16)))
    place = lax.broadcasted_iota(jnp.int32, (row_count, 1), 0) + me * row_count + 1
    counted = jnp.minimum(place, span).astype(f32)
    diff = (total / counted - joined[reach:]).astype(bf16)
    pooled[...] = (
        jnp.dot(diff, mix[...], preferred_element_type=f32) * gain[...]
    ).astype(bf16)

    def project(yy, cc):
        span = pl.ds(block(yy, cc), tokens)

        @pl.loop(0, front)
        def _(h):
            part[span, fcols(h)] = jnp.dot(
                pooled[span, :], proj[:, fcols(h)], preferred_element_type=f32
            ).astype(bf16)

    for yy, place in ((1 - y, 0), (y, 1)):
        project(yy, 1 - c)

        @pl.loop(0, pieces)
        def _(k):
            pair_copy(yy, place, k).start()

        project(yy, c)

    @pl.loop(1, 8)
    def _(q):
        meta_copy(q).start()

    @pl.loop(0, pieces)
    def _(k):
        pair_copy(1 - y, 0, k).wait_recv()
        far_out[piece(k)] = (
            part[block_piece(1 - y, c, k)].astype(f32) + pair_in[0, piece(k)].astype(f32)
        ).astype(bf16)
        far_copy(k).start()

    @pl.loop(0, pieces)
    def _(k):
        pair_copy(y, 1, k).wait_recv()
        far_copy(k).wait_recv()
        added = (
            part[block_piece(y, c, k)].astype(f32)
            + pair_in[1, piece(k)].astype(f32)
            + far_in[piece(k)].astype(f32)
        ).astype(bf16)
        values = stay[piece(k)].astype(f32) + added.astype(f32)
        mixed[piece(k)] = values
        scale = lax.rsqrt(jnp.mean(values * values, axis=1, keepdims=True) + EPS)
        rows[z, piece(k)] = (values * scale * scales[...]).astype(bf16)
        pass_copy(z, k, z1, ra_send).start()

        @pl.when(mid)
        def _():
            pass_copy(z, k, z2, rb_send).start()

    def picks_of(zt):
        places = meta[zt, y, :experts, :]
        level = lax.broadcasted_iota(jnp.int32, places.shape, 0)
        slot = lax.broadcasted_iota(jnp.int32, (C, tokens), 0).astype(f32)

        def one(expert):
            place = jnp.sum(jnp.where(level == expert, places, 0.0), axis=0, keepdims=True)
            return jnp.where(place[:, :tokens] == slot, 1.0, 0.0)

        return jnp.concatenate([one(me), one(peer_expert)], axis=0).astype(bf16)

    def gather(picks, zt, h):
        found = jnp.dot(picks, rows[zt, :, fcols(h)], preferred_element_type=f32)
        found = found.astype(bf16)
        give[zt, :, fcols(h)] = found[C:]
        xf_copy(zt, h).start()
        slots[zt, spot(x, y), fcols(h)] = found[:C]
        yf_copy(zt, x, h).start()

    def arrive(zt, onward):
        meta_here(zt, y)
        picks = picks_of(zt)

        @pl.loop(0, pieces)
        def _(k):
            pass_copy(zt, k, z1, ra_send).wait_recv()
            onward(k)

        @pl.loop(0, front)
        def _(h):
            gather(picks, zt, h)

    def nothing(h):
        pass

    def turn(zt):
        @pl.loop(0, front)
        def _(h):
            xf_copy(zt, h).wait_recv()
            yf_copy(zt, 1 - x, h).start()

    def complete(zt):
        @pl.loop(0, front)
        def _(h):
            yf_copy(zt, x, h).wait_recv()
            yf_copy(zt, 1 - x, h).wait_recv()
            mf_copy(zt, h).start()

    def compute(zt):
        @pl.loop(0, front)
        def _(h):
            mf_copy(zt, h).wait_recv()

        v = slots[zt]
        gate = jnp.dot(v, wg[...], preferred_element_type=f32)
        upper = jnp.dot(v, wu[...], preferred_element_type=f32)
        hidden = (gate * (1.0 / (1.0 + jnp.exp(-gate))) * upper).astype(bf16)

        @pl.loop(0, back)
        def _(h):
            parts[zt, :, bcols(h)] = jnp.dot(
                hidden, wd[:, bcols(h)], preferred_element_type=f32
            ).astype(bf16)
            mb_copy(zt, h).start()

    def pair_sum(zt, far, first=0, stop=back):
        @pl.loop(first, stop)
        def _(h):
            mb_copy(zt, h).wait_recv()
            total = (
                parts[zt, half(c), bcols(h)].astype(f32) + mate_in[zt, :, bcols(h)].astype(f32)
            )
            parts[zt, half(c), bcols(h)] = total.astype(bf16)
            if far:
                yb_copy(zt, 0, h).start()
                yb_copy(zt, 1, h).start()
            else:
                xb_copy(zt, True, h).start()

    def far_piece(zt, h):
        for xx in (0, 1):
            yb_copy(zt, xx, h).wait_recv()
            total = (
                parts[zt, spot(xx, y), bcols(h)].astype(f32)
                + y_in[zt, strip(xx), bcols(h)].astype(f32)
            )
            parts[zt, spot(xx, y), bcols(h)] = total.astype(bf16)
        xb_copy(zt, False, h).start()

    def far_sum(zt):
        @pl.loop(0, back)
        def _(h):
            far_piece(zt, h)

    def weights_of(zt, yt):
        places = meta[zt, yt, :experts, :]
        shares = meta[zt, yt, experts:, :]
        level = lax.broadcasted_iota(jnp.int32, places.shape, 0)
        slot = lax.broadcasted_iota(jnp.int32, (C, places.shape[1]), 0).astype(f32)

        def one(expert):
            place = jnp.sum(jnp.where(level == expert, places, 0.0), axis=0, keepdims=True)
            share = jnp.sum(jnp.where(level == expert, shares, 0.0), axis=0, keepdims=True)
            spread = jnp.where(place == slot, share, 0.0)
            head = spread.astype(bf16).astype(f32)
            return head, spread - head

        mine, theirs = one(me), one(peer_expert)
        both = jnp.concatenate([mine[0], theirs[0], mine[1], theirs[1]], axis=0)
        return both.T[:tokens].astype(bf16)

    def blend(spread, zt, yt, h):
        mine = parts[zt, spot(x, yt), bcols(h)]
        theirs = x_in[zt, strip(yt), bcols(h)]
        pair = jnp.concatenate([mine, theirs, mine, theirs], axis=0)
        return jnp.dot(spread, pair, preferred_element_type=f32)

    def near_other(zt, side, first=0, stop=back):
        there = weights_of(zt, 1 - y)

        @pl.loop(first, stop)
        def _(h):
            xb_copy(zt, True, h).wait_recv()
            sums[zt, 1 - y, :, bcols(h)] = blend(there, zt, 1 - y, h).astype(bf16)
            home_copy(zt, 1 - y, side, h).start()

    def near_same(zt, side, first=0, stop=back):
        here = weights_of(zt, y)

        @pl.loop(first, stop)
        def _(h):
            total = blend(here, zt, y, h)

            @pl.when(mid)
            def _():
                line_copy(zt, h, z1).wait_recv()
                sums[zt, y, :, bcols(h)] = (
                    total + line_in[zt, :, bcols(h)].astype(f32)
                ).astype(bf16)

            @pl.when(end)
            def _():
                sums[zt, y, :, bcols(h)] = total.astype(bf16)

            home_copy(zt, y, side, h).start()

    def far_back():
        mixes[0] = weights_of(z3, y)
        mixes[1] = weights_of(z1, y)

        @pl.loop(0, back + LAG)
        def _(i):
            @pl.when(i < back)
            def _():
                xb_copy(z3, False, i).wait_recv()
                total = blend(mixes[0], z3, y, i)
                line_copy(z3, i, z1).wait_recv()
                sums[z3, y, :, bcols(i)] = (
                    total + line_in[z3, :, bcols(i)].astype(f32)
                ).astype(bf16)
                line_copy(z3, i, z2).start()

            @pl.when(i >= LAG)
            def _():
                k = i - LAG
                total = blend(mixes[1], z1, y, k)
                line_copy(z1, k, z1).wait_recv()
                sums[z1, y, :, bcols(k)] = (
                    total + line_in[z1, :, bcols(k)].astype(f32)
                ).astype(bf16)
                home_copy(z1, y, 0, k).start()

    def far_chain():
        mixes[0] = weights_of(z2, y)
        mixes[1] = weights_of(z3, y)

        @pl.loop(0, 2 * back + LAG)
        def _(i):
            @pl.when(i < 2 * back)
            def _():
                far_piece(z2 + (z3 - z2) * (i // back), i % back)

            @pl.when(i >= LAG)
            def _():
                k = i - LAG
                which, h = k // back, k % back
                zt = z2 + (z3 - z2) * which
                xb_copy(zt, False, h).wait_recv()
                sums[zt, y, :, bcols(h)] = blend(mixes[which], zt, y, h).astype(bf16)
                line_copy(zt, h, z1).start()

    def own_back():
        here = weights_of(z, y)
        there = weights_of(z, 1 - y)

        @pl.loop(0, back)
        def _(h):
            xb_copy(z, True, h).wait_recv()
            sums[z, 1 - y, :, bcols(h)] = blend(there, z, 1 - y, h).astype(bf16)
            mixed[:, bcols(h)] += blend(here, z, y, h)

    def last_send():
        @pl.loop(0, back)
        def _(h):
            home_here(1 - y, 0, h)
            total = (
                sums[z, 1 - y, :, bcols(h)].astype(f32) + home_in[0, 1 - y, :, bcols(h)].astype(f32)
            )

            @pl.when(mid)
            def _():
                home_here(1 - y, 1, h)
                sums[z, 1 - y, :, bcols(h)] = (
                    total + home_in[1, 1 - y, :, bcols(h)].astype(f32)
                ).astype(bf16)

            @pl.when(end)
            def _():
                sums[z, 1 - y, :, bcols(h)] = total.astype(bf16)

            last_copy(h).start()

    def finish():
        @pl.loop(0, back)
        def _(h):
            home_here(y, 0, h)
            last_copy(h).wait_recv()
            total = (
                mixed[:, bcols(h)]
                + home_in[0, y, :, bcols(h)].astype(f32)
                + last_in[:, bcols(h)].astype(f32)
            )

            @pl.when(mid)
            def _():
                home_here(y, 1, h)
                out[:, bcols(h)] = (total + home_in[1, y, :, bcols(h)].astype(f32)).astype(bf16)

            @pl.when(end)
            def _():
                out[:, bcols(h)] = total.astype(bf16)

    def scoped(fn, name):
        def run(*args):
            with jax.named_scope(name):
                fn(*args)
        return run

    arrive = scoped(arrive, "arrive")
    turn = scoped(turn, "turn")
    complete = scoped(complete, "complete")
    compute = scoped(compute, "compute")
    pair_sum = scoped(pair_sum, "pair_sum")
    far_sum = scoped(far_sum, "far_sum")
    near_other = scoped(near_other, "near_other")
    near_same = scoped(near_same, "near_same")
    far_back = scoped(far_back, "far_back")
    own_back = scoped(own_back, "own_back")
    last_send = scoped(last_send, "last_send")
    far_chain = scoped(far_chain, "far_chain")

    def onto(zt, to, send):
        return lambda h: pass_copy(zt, h, to, send).start()

    def first_on(h):
        @pl.when(mid)
        def _():
            pass_copy(z1, h, z2, rb_send).start()

    meta_picks = picks_of(z)

    @pl.loop(0, front)
    def _(h):
        gather(meta_picks, z, h)

    turn(z)
    arrive(z1, first_on)

    @pl.when(mid)
    def _():
        arrive(z2, onto(z2, z1, ra_send))

    turn(z1)

    @pl.when(mid)
    def _():
        turn(z2)
        arrive(z3, onto(z3, z1, ra_send))

    complete(z)
    for zt in (z, z1, z2, z3):
        meta_here(zt, 1 - y)
    for load in loads:
        load.wait()
    compute(z)

    @pl.when(end)
    def _():
        arrive(z2, nothing)

    complete(z1)
    compute(z1)

    @pl.when(end)
    def _():
        turn(z2)
        pair_sum(z1, False, 0, back // 2)
        arrive(z3, nothing)
        pair_sum(z1, False, back // 2, back)
        near_other(z1, 0, 0, back // 2)

    @pl.when(mid)
    def _():
        turn(z3)
        pair_sum(z1, False)

    complete(z2)
    compute(z2)

    @pl.when(end)
    def _():
        turn(z3)
        pair_sum(z2, True)
        near_other(z1, 0, back // 2, back)
        near_same(z1, 0)
        pair_sum(z, False)

    @pl.when(mid)
    def _():
        pair_sum(z2, False)

    complete(z3)
    compute(z3)
    pair_sum(z3, True)

    @pl.when(end)
    def _():
        far_chain()
        own_back()
        last_send()

    @pl.when(mid)
    def _():
        pair_sum(z, False)
        near_other(z1, 0)
        near_other(z2, 1)
        far_sum(z3)
        own_back()
        last_send()
        near_same(z2, 1)
        far_back()

    with jax.named_scope("finish"):
        finish()

    @pl.loop(1, 8)
    def _(q):
        meta_copy(q).wait_send()

    @pl.when(me < count - 1)
    def _():
        halo_copy().wait_send()

    pair_copy(1 - y, 0, None).wait_send()
    pair_copy(y, 1, None).wait_send()
    far_copy(None).wait_send()
    pass_copy(z, None, z1, ra_send).wait_send()
    for zt in (z, z1, z2, z3):
        xf_copy(zt, None).wait_send()
        yf_copy(zt, 0, None).wait_send()
        yf_copy(zt, 1, None).wait_send()
        mf_copy(zt, None).wait_send()
        mb_copy(zt, None).wait_send()
    xb_copy(z, True, None).wait_send()
    xb_copy(z1, True, None).wait_send()
    xb_copy(z3, False, None).wait_send()
    yb_copy(z3, 0, None).wait_send()
    yb_copy(z3, 1, None).wait_send()
    line_copy(z3, None, z1).wait_send()
    home_copy(z1, 0, 0, None).wait_send()
    home_copy(z1, 1, 0, None).wait_send()
    last_copy(None).wait_send()

    @pl.when(mid)
    def _():
        pass_copy(z, None, z2, rb_send).wait_send()
        pass_copy(z1, None, z2, rb_send).wait_send()
        pass_copy(z2, None, z1, ra_send).wait_send()
        pass_copy(z3, None, z1, ra_send).wait_send()
        xb_copy(z2, True, None).wait_send()
        home_copy(z2, 0, 1, None).wait_send()
        home_copy(z2, 1, 1, None).wait_send()

    @pl.when(end)
    def _():
        xb_copy(z2, False, None).wait_send()
        yb_copy(z2, 0, None).wait_send()
        yb_copy(z2, 1, None).wait_send()
        line_copy(z2, None, z1).wait_send()


FRONT, BACK, LAG = 4, 4, 2


def layer_kernel(
    resid, pool_in, pool_mix, pool_gain, out_proj, norm_gain,
    w_gate, w_up, w_down, routes, route_weight, capacity, experts, slices,
):
    row_count, width = resid.shape
    tokens = row_count // slices
    channels = pool_in.shape[1]
    units = w_gate.shape[2]
    bf16, f32 = jnp.bfloat16, jnp.float32
    dma = pltpu.SemaphoreType.DMA
    C = capacity
    vmem = pltpu.VMEM
    pieces = tokens // 16

    def lanes(*shape, pieces):
        return [dma(shape), dma(shape + (pieces,))]

    return pl.pallas_call(
        functools.partial(moe_kernel, FRONT, BACK, capacity, experts),
        out_shape=jax.ShapeDtypeStruct((tokens, width), bf16),
        in_specs=[pl.BlockSpec(memory_space=pl.ANY)] * 11,
        out_specs=pl.BlockSpec(memory_space=pltpu.VMEM),
        scratch_shapes=[
            vmem((row_count, channels), bf16),
            vmem((channels, channels), bf16),
            vmem((1, channels), f32),
            vmem((channels, width), bf16),
            vmem((1, width), f32),
            vmem((2, row_count), jnp.int32),
            vmem((2, row_count), f32),
            vmem((tokens, width), bf16),
            vmem((2**GROUPS, channels), bf16),
            vmem((row_count, channels), bf16),
            vmem((row_count, width), bf16),
            vmem((2, tokens, width), bf16),
            vmem((tokens, width), bf16),
            vmem((tokens, width), bf16),
            vmem((tokens, width), f32),
            vmem((2 * experts, 128), f32),
            vmem((width, units), bf16),
            vmem((width, units), bf16),
            vmem((units, width), bf16),
            vmem((4, tokens, width), bf16),
            vmem((4, 2, 2 * experts, 128), f32),
            vmem((4, 8 * C, width), bf16),
            vmem((4, C, width), bf16),
            vmem((4, 8 * C, width), bf16),
            vmem((4, 4 * C, width), bf16),
            vmem((4, 2 * C, width), bf16),
            vmem((4, 2 * C, width), bf16),
            vmem((4, 2, tokens, width), bf16),
            vmem((4, tokens, width), bf16),
            vmem((2, 2, tokens, width), bf16),
            vmem((tokens, width), bf16),
            vmem((2, tokens, 4 * C), bf16),
            dma((11,)), dma, dma, dma((2,)), dma((2, pieces)), dma, dma((pieces,)),
            dma((8,)), dma((4, 2)), dma((4, pieces)), dma((4,)), dma((4,)),
        ]
        + lanes(4, pieces=FRONT) + lanes(4, 2, pieces=FRONT) + lanes(4, pieces=FRONT)
        + lanes(4, pieces=BACK) + lanes(4, 2, pieces=BACK) + lanes(4, pieces=BACK)
        + lanes(4, pieces=BACK) + lanes(2, 2, pieces=BACK) + [dma, dma((BACK,))],
        compiler_params=pltpu.CompilerParams(
            collective_id=1, has_side_effects=True, vmem_limit_bytes=63 * 2**20
        ),
        cost_estimate=pl.CostEstimate(
            flops=6 * experts * 4 * C * width * units,
            bytes_accessed=4 * 2 * width * units,
            transcendentals=0,
        ),
        name="moe_exchange",
    )(
        resid, pool_in, pool_mix, pool_gain[None], out_proj, norm_gain[None],
        w_gate, w_up, w_down, routes.T, route_weight.T,
    )


def sum_kernel(count, part, out, pair_in, total, y_in, pp_send, pp_recv, y_send, y_recv):
    me = lax.axis_index("sp")
    tp = lax.axis_index("tp")
    core, y = tp % 2, tp // 2
    mate = y * 2 + (1 - core)
    across = (1 - y) * 2 + core
    pieces = count // 16
    mesh_id = pl.DeviceIdType.MESH
    barrier = pltpu.get_barrier_semaphore()
    for peer in (mate, across):
        pl.semaphore_signal(barrier, inc=1, device_id=(me, peer), device_id_type=mesh_id)
    pl.semaphore_wait(barrier, 2)

    def at(yy, c, k):
        return pl.ds(pl.multiple_of((yy * 2 + c) * count + k * 16, 16), 16)

    def piece(k):
        return pl.ds(pl.multiple_of(k * 16, 16), 16)

    def pair_copy(yy, k, place):
        return pltpu.make_async_remote_copy(
            src_ref=part.at[at(yy, 1 - core, k)], dst_ref=pair_in.at[place, piece(k)],
            send_sem=pp_send.at[place, k], recv_sem=pp_recv.at[place, k],
            device_id=(me, mate), device_id_type=mesh_id,
        )

    def far_copy(k):
        return pltpu.make_async_remote_copy(
            src_ref=total.at[piece(k)], dst_ref=y_in.at[piece(k)],
            send_sem=y_send.at[k], recv_sem=y_recv.at[k],
            device_id=(me, across), device_id_type=mesh_id,
        )

    @pl.loop(0, pieces)
    def _(k):
        pair_copy(1 - y, k, 0).start()

    @pl.loop(0, pieces)
    def _(k):
        pair_copy(y, k, 1).start()

    @pl.loop(0, pieces)
    def _(k):
        pair_copy(1 - y, k, 0).wait_recv()
        total[piece(k)] = (
            part[at(1 - y, core, k)].astype(jnp.float32)
            + pair_in[0, piece(k)].astype(jnp.float32)
        ).astype(jnp.bfloat16)
        far_copy(k).start()

    @pl.loop(0, pieces)
    def _(k):
        pair_copy(y, k, 1).wait_recv()
        far_copy(k).wait_recv()
        out[piece(k)] = (
            part[at(y, core, k)].astype(jnp.float32)
            + pair_in[1, piece(k)].astype(jnp.float32)
            + y_in[piece(k)].astype(jnp.float32)
        ).astype(jnp.bfloat16)

    @pl.loop(0, pieces)
    def _(k):
        pair_copy(1 - y, k, 0).wait_send()
        pair_copy(y, k, 1).wait_send()
        far_copy(k).wait_send()


def scatter_sum(part, slices):
    row_count, width = part.shape
    count = row_count // slices
    pieces = count // 16
    bf16 = jnp.bfloat16
    dma = pltpu.SemaphoreType.DMA
    return pl.pallas_call(
        functools.partial(sum_kernel, count),
        out_shape=jax.ShapeDtypeStruct((count, width), bf16),
        in_specs=[pl.BlockSpec(memory_space=pltpu.VMEM)],
        out_specs=pl.BlockSpec(memory_space=pltpu.VMEM),
        scratch_shapes=[
            pltpu.VMEM((2, count, width), bf16),
            pltpu.VMEM((count, width), bf16),
            pltpu.VMEM((count, width), bf16),
            dma((2, pieces)),
            dma((2, pieces)),
            dma((pieces,)),
            dma((pieces,)),
        ],
        compiler_params=pltpu.CompilerParams(
            collective_id=2, has_side_effects=True, vmem_limit_bytes=24 * 2**20
        ),
        cost_estimate=pl.CostEstimate(flops=0, bytes_accessed=2**25, transcendentals=0),
        name="scatter_sum",
    )(part)


def on_device(
    resid,
    pool_in,
    pool_mix,
    pool_gain,
    out_proj,
    norm_gain,
    w_gate,
    w_up,
    w_down,
    routes,
    route_weight,
):
    token_count, width = resid.shape
    choose = routes.shape[1]
    experts = lax.axis_size("sp")
    slices = lax.axis_size("tp")
    sub_count = token_count // slices
    capacity = max(2, 2 * sub_count * choose // experts)
    whole = experts == 8 and slices == 4 and choose == 2 and token_count % 16 == 0
    if whole and sub_count == 2 * capacity and 4 * capacity == 128:
        return layer_kernel(
            resid, pool_in, pool_mix, pool_gain, out_proj, norm_gain,
            w_gate, w_up, w_down, routes, route_weight, capacity, experts, slices,
        )
    tp_index = lax.axis_index("tp")
    diff = group_diff(pool_in)
    pooled = (jnp.dot(diff, pool_mix[0], preferred_element_type=jnp.float32) * pool_gain).astype(
        jnp.bfloat16
    )
    group_part = rounded(jnp.dot(pooled, out_proj, preferred_element_type=jnp.float32)).astype(
        jnp.bfloat16
    )
    if slices == 4 and sub_count % 16 == 0:
        proj = scatter_sum(group_part, slices).astype(jnp.float32)
    else:
        proj = rounded(
            lax.psum_scatter(group_part, "tp", scatter_dimension=0, tiled=True).astype(jnp.float32)
        )
    first = tp_index * sub_count
    mixed = lax.dynamic_slice_in_dim(resid, first, sub_count, 0).astype(jnp.float32) + proj
    normed = normalize(mixed, norm_gain)
    route_rows = lax.dynamic_slice_in_dim(routes, first, sub_count, 0)
    weight_rows = lax.dynamic_slice_in_dim(route_weight, first, sub_count, 0)
    targets = slot_plan(route_rows, 1, capacity, experts)
    outgoing = fill_slots(normed, targets, experts * capacity)
    outgoing = outgoing.reshape(experts, capacity, width)
    arrived = lax.all_to_all(outgoing, "sp", split_axis=0, concat_axis=0, tiled=True)
    block_rows = lax.all_gather(arrived, "tp", axis=0, tiled=True)
    spread = expert_part(block_rows.reshape(-1, width), w_gate, w_up, w_down).reshape(
        block_rows.shape
    )
    stacked = spread.reshape((slices,) + arrived.shape)
    received = lax.all_to_all(stacked, "tp", split_axis=0, concat_axis=0, tiled=True)
    summed = jnp.sum(received.astype(jnp.float32), axis=0)
    returned = lax.all_to_all(
        summed.astype(jnp.bfloat16), "sp", split_axis=0, concat_axis=0, tiled=True
    )
    moe = collect(returned.reshape(-1, width), targets, weight_rows)
    return (mixed + moe).astype(jnp.bfloat16)


def solution(mesh):
    in_specs = (
        P("sp", None),
        P("sp", "tp"),
        P("tp", None, None),
        P("tp"),
        P("tp", None),
        P(),
        P("sp", None, "tp"),
        P("sp", None, "tp"),
        P("sp", "tp", None),
        P("sp", None),
        P("sp", None),
    )
    out_specs = P(("sp", "tp"), None)
    return jax.shard_map(
        on_device, mesh=mesh, in_specs=in_specs, out_specs=out_specs, check_vma=False
    )
```

```python
import functools

import jax
import jax.numpy as jnp
from jax import lax
from jax.experimental import pallas as pl
from jax.experimental.pallas import tpu as pltpu
from jax.sharding import PartitionSpec as P

GROUPS = 4


EPS = 1e-06


def shifted(x, axis, by):
    count = lax.axis_size(axis)
    pairs = [(i, i + by) for i in range(count) if 0 <= i + by < count]
    return lax.ppermute(x, axis, pairs)


def rounded(value):
    return lax.optimization_barrier(value.astype(jnp.bfloat16)).astype(jnp.float32)


def group_diff(pool_in):
    row_count = pool_in.shape[0]
    reach = 2**GROUPS
    before = shifted(pool_in[row_count - reach :], "sp", 1)
    joined = jnp.concatenate([before, pool_in], axis=0).astype(jnp.float32)
    running = jnp.cumsum(joined, axis=0)
    width = jnp.left_shift(jnp.int32(2), lax.axis_index("tp"))
    lagged = lax.dynamic_slice_in_dim(running, reach - width, row_count, 0)
    total = running[reach:] - lagged
    place = lax.axis_index("sp") * row_count + jnp.arange(row_count, dtype=jnp.int32) + 1
    counted = jnp.minimum(place, width).astype(jnp.float32)
    return (total / counted[:, None] - joined[reach:]).astype(jnp.bfloat16)


def normalize(mixed, norm_gain):
    scale = lax.rsqrt(jnp.mean(mixed * mixed, axis=1, keepdims=True) + EPS)
    return (mixed * scale * norm_gain).astype(jnp.bfloat16)


def slot_plan(route_rows, blocks, capacity, experts):
    row_count, choose = route_rows.shape
    flat_routes = route_rows.reshape(blocks, row_count // blocks * choose)
    onehot = (
        flat_routes[:, :, None] == jnp.arange(experts, dtype=jnp.int32)[None, None, :]
    ).astype(jnp.int32)
    earlier = jnp.cumsum(onehot, axis=1) - onehot
    position = jnp.sum(earlier * onehot, axis=2)
    block_ids = jnp.arange(blocks, dtype=jnp.int32)[:, None]
    return (flat_routes * (blocks * capacity) + block_ids * capacity + position).reshape(-1)


def fill_slots(normed, targets, slot_count):
    row_count, width = normed.shape
    slots = jnp.arange(slot_count, dtype=jnp.int32)[:, None, None]
    picks = jnp.sum((targets.reshape(row_count, -1)[None] == slots).astype(jnp.bfloat16), axis=2)
    return jnp.dot(picks, normed, preferred_element_type=jnp.float32).astype(normed.dtype)


def collect(returned, targets, weights):
    row_count, choose = weights.shape
    slots = jnp.arange(returned.shape[0], dtype=jnp.int32)[None, None, :]
    chosen = targets.reshape(row_count, choose)[:, :, None] == slots
    spread = jnp.sum(jnp.where(chosen, weights[:, :, None], 0.0), axis=1)
    head = lax.reduce_precision(spread, 8, 7)
    tail = spread - head
    both = jnp.concatenate([head, tail], axis=0).astype(jnp.bfloat16)
    product = jnp.dot(both, returned, preferred_element_type=jnp.float32)
    return product[:row_count] + product[row_count:]


def expert_part(inputs, w_gate, w_up, w_down):
    gate = jnp.dot(inputs, w_gate[0], preferred_element_type=jnp.float32)
    upper = jnp.dot(inputs, w_up[0], preferred_element_type=jnp.float32)
    hidden = (jax.nn.silu(gate) * upper).astype(jnp.bfloat16)
    return jnp.dot(hidden, w_down[0], preferred_element_type=jnp.float32).astype(jnp.bfloat16)


def line_plan(z):
    first = z + 1 - 2 * (z % 2)
    second = 2 - z // 2
    third = 3 - 3 * (z // 2)
    return first, second, third


def moe_kernel(
    front, back, capacity, experts,
    resid, pool_in, pool_mix, pool_gain, out_proj, norm_gain,
    wg_hbm, wu_hbm, wd_hbm, routes, shares_in, out,
    pool, mix, gain, proj, scales, named, shares, stay, halo, pooled, part,
    pair_in, far_out, far_in, mixed, meta_in,
    wg, wu, wd, rows, meta, slots, give, parts,
    mate_in, y_in, x_in, sums, line_in, home_in, last_in, mixes,
    w_sem, h_send, h_recv, pp_send, pp_recv, fy_send, fy_recv,
    m_send, m_recv, r_recv, ra_send, rb_send,
    xf_send, xf_recv, yf_send, yf_recv, mf_send, mf_recv,
    mb_send, mb_recv, yb_send, yb_recv, xb_send, xb_recv,
    zf_send, zf_recv, zh_send, zh_recv, yl_send, yl_recv,
):
    me = lax.axis_index("sp")
    tp = lax.axis_index("tp")
    z, x = me // 2, me % 2
    y, c = tp // 2, tp % 2
    C = capacity
    tokens, width = out.shape
    count = lax.axis_size("sp")
    row_count = pool.shape[0]
    reach = halo.shape[0]
    first = pl.multiple_of(tp * tokens, tokens)
    pieces = tokens // 16
    wf, wb = width // front, width // back
    z1, z2, z3 = line_plan(z)
    mid = ((z + 1) // 2) % 2 == 1
    end = ((z + 1) // 2) % 2 == 0
    mate = (me, y * 2 + 1 - c)
    across = (me, (1 - y) * 2 + c)
    peer_expert = me + 1 - 2 * x
    beside = (peer_expert, tp)
    f32, bf16 = jnp.float32, jnp.bfloat16

    def plane(zz):
        return (zz * 2 + x, tp)

    def remote(src, dst, send, recv, to):
        return pltpu.make_async_remote_copy(
            src_ref=src, dst_ref=dst, send_sem=send, recv_sem=recv,
            device_id=to, device_id_type=pl.DeviceIdType.MESH,
        )

    def fcols(h):
        if h is None:
            return pl.ds(0, width)
        return pl.ds(pl.multiple_of(h * wf, wf), wf)

    def bcols(h):
        if h is None:
            return pl.ds(0, width)
        return pl.ds(pl.multiple_of(h * wb, wb), wb)

    def spot(xx, yy):
        return pl.ds(pl.multiple_of(c * 4 * C + xx * 2 * C + yy * C, C), C)

    def both(xx):
        return pl.ds(pl.multiple_of(c * 4 * C + xx * 2 * C, 2 * C), 2 * C)

    def half(cc):
        return pl.ds(pl.multiple_of(cc * 4 * C, 4 * C), 4 * C)

    def strip(yy):
        return pl.ds(pl.multiple_of(yy * C, C), C)

    def meta_copy(q):
        zq, yq = (z + q // 2) % 4, (y + q) % 2
        return remote(meta_in, meta.at[z, y], m_send.at[q], m_recv.at[z, y],
                      (zq * 2 + x, yq * 2 + c))

    def meta_here(zt, yt):
        remote(meta.at[zt, yt], meta.at[zt, yt], m_send.at[0], m_recv.at[zt, yt],
               mate).wait_recv()

    def at(h):
        return 0 if h is None else h

    def piece(k):
        if k is None:
            return pl.ds(0, tokens)
        return pl.ds(pl.multiple_of(k * 16, 16), 16)

    def block(yy, cc):
        return pl.multiple_of((yy * 2 + cc) * tokens, tokens)

    def block_piece(yy, cc, k):
        return pl.ds(pl.multiple_of(block(yy, cc) + k * 16, 16), 16)

    def halo_copy():
        return remote(pool.at[pl.ds(row_count - reach, reach)], halo, h_send, h_recv,
                      (me + 1, tp))

    def pair_copy(yy, place, k):
        if k is None:
            return remote(part.at[pl.ds(block(yy, 1 - c), tokens)], pair_in.at[place],
                          pp_send.at[place], pp_recv.at[place, 0], mate)
        return remote(part.at[block_piece(yy, 1 - c, k)], pair_in.at[place, piece(k)],
                      pp_send.at[place], pp_recv.at[place, k], mate)

    def far_copy(k):
        return remote(far_out.at[piece(k)], far_in.at[piece(k)],
                      fy_send, fy_recv.at[at(k)], across)

    def pass_copy(zt, h, to, send):
        ref = rows.at[zt, piece(h)]
        return remote(ref, ref, send.at[zt], r_recv.at[zt, at(h)], plane(to))

    def xf_copy(zt, h):
        return remote(give.at[zt, :, fcols(h)], slots.at[zt, spot(x, y), fcols(h)],
                      xf_send.at[zt], xf_recv.at[zt, at(h)], beside)

    def yf_copy(zt, xx, h):
        ref = slots.at[zt, spot(xx, y), fcols(h)]
        return remote(ref, ref, yf_send.at[zt, xx], yf_recv.at[zt, xx, at(h)], across)

    def mf_copy(zt, h):
        ref = slots.at[zt, half(c), fcols(h)]
        return remote(ref, ref, mf_send.at[zt], mf_recv.at[zt, at(h)], mate)

    def mb_copy(zt, h):
        return remote(parts.at[zt, half(1 - c), bcols(h)], mate_in.at[zt, :, bcols(h)],
                      mb_send.at[zt], mb_recv.at[zt, at(h)], mate)

    def yb_copy(zt, xx, h):
        return remote(parts.at[zt, spot(xx, 1 - y), bcols(h)], y_in.at[zt, strip(xx), bcols(h)],
                      yb_send.at[zt, xx], yb_recv.at[zt, xx, at(h)], across)

    def xb_copy(zt, near, h):
        if near:
            return remote(parts.at[zt, both(1 - x), bcols(h)], x_in.at[zt, :, bcols(h)],
                          xb_send.at[zt], xb_recv.at[zt, at(h)], beside)
        return remote(parts.at[zt, spot(1 - x, y), bcols(h)], x_in.at[zt, strip(y), bcols(h)],
                      xb_send.at[zt], xb_recv.at[zt, at(h)], beside)

    def line_copy(zt, h, to):
        return remote(sums.at[zt, y, :, bcols(h)], line_in.at[zt, :, bcols(h)],
                      zf_send.at[zt], zf_recv.at[zt, at(h)], plane(to))

    def home_copy(zt, yt, side, h):
        return remote(sums.at[zt, yt, :, bcols(h)], home_in.at[side, yt, :, bcols(h)],
                      zh_send.at[side, yt], zh_recv.at[side, yt, at(h)], plane(zt))

    def home_here(yt, side, h):
        ref = home_in.at[side, yt, :, bcols(h)]
        remote(ref, ref, zh_send.at[side, yt], zh_recv.at[side, yt, at(h)], mate).wait_recv()

    def last_copy(h):
        return remote(sums.at[z, 1 - y, :, bcols(h)], last_in.at[:, bcols(h)],
                      yl_send, yl_recv.at[at(h)], across)

    small = [
        pltpu.make_async_copy(pool_in, pool, w_sem.at[3]),
        pltpu.make_async_copy(routes, named, w_sem.at[4]),
        pltpu.make_async_copy(shares_in, shares, w_sem.at[5]),
        pltpu.make_async_copy(pool_mix.at[0], mix, w_sem.at[6]),
        pltpu.make_async_copy(pool_gain, gain, w_sem.at[7]),
        pltpu.make_async_copy(out_proj, proj, w_sem.at[8]),
        pltpu.make_async_copy(resid.at[pl.ds(first, tokens)], stay, w_sem.at[9]),
        pltpu.make_async_copy(norm_gain, scales, w_sem.at[10]),
    ]
    loads = [
        pltpu.make_async_copy(wg_hbm.at[0], wg, w_sem.at[0]),
        pltpu.make_async_copy(wu_hbm.at[0], wu, w_sem.at[1]),
        pltpu.make_async_copy(wd_hbm.at[0], wd, w_sem.at[2]),
    ]
    for load in small + loads:
        load.start()

    barrier = pltpu.get_barrier_semaphore()
    for peer in (mate, beside):
        pl.semaphore_signal(barrier, inc=1, device_id=peer,
                            device_id_type=pl.DeviceIdType.MESH)

    @pl.when(me > 0)
    def _():
        pl.semaphore_signal(barrier, inc=1, device_id=(me - 1, tp),
                            device_id_type=pl.DeviceIdType.MESH)

    @pl.loop(1, 8)
    def _(q):
        zq, yq = (z + q // 2) % 4, (y + q) % 2
        pl.semaphore_signal(barrier, inc=1, device_id=(zq * 2 + x, yq * 2 + c),
                            device_id_type=pl.DeviceIdType.MESH)

    pl.semaphore_wait(barrier, 9 + (2 * count - 2 - me) // count)
    small[0].wait()

    @pl.when(me < count - 1)
    def _():
        halo_copy().start()

    for load in small[1:]:
        load.wait()

    level = lax.broadcasted_iota(jnp.int32, (experts, row_count), 0)
    one_is, two_is = named[0:1, :] == level, named[1:2, :] == level
    hit = jnp.where(one_is | two_is, 1.0, 0.0)
    share = jnp.where(one_is, shares[0:1, :], 0.0) + jnp.where(two_is, shares[1:2, :], 0.0)
    head = share.astype(bf16).astype(f32)
    stack = jnp.concatenate([hit, head, share - head, hit], axis=0).astype(bf16)
    row = lax.broadcasted_iota(jnp.int32, (row_count, 128), 0)
    lane = lax.broadcasted_iota(jnp.int32, (row_count, 128), 1)
    inside = lane < tokens
    here = jnp.where((row == lane + first) & inside, 1.0, 0.0).astype(bf16)
    ahead = jnp.where((row >= first) & (row < lane + first) & inside, 1.0, 0.0).astype(bf16)
    taken = jnp.dot(stack, here, preferred_element_type=f32)
    before = jnp.dot(stack, ahead, preferred_element_type=f32)
    table = jnp.concatenate(
        [
            jnp.where(taken[:experts] > 0.5, before[:experts], -1.0),
            taken[experts:2 * experts] + taken[2 * experts:3 * experts],
        ],
        axis=0,
    )
    meta_in[...] = table
    meta[z, y] = table

    def pool_rows(joined, first_place):
        runs = [joined.astype(f32)]
        for by in (1, 2, 4, 8):
            runs.append(runs[-1] + pltpu.roll(runs[-1], by, 0))
        total = jnp.where(
            tp == 0, runs[1], jnp.where(tp == 1, runs[2], jnp.where(tp == 2, runs[3], runs[4]))
        )[reach:]
        span = jnp.where(tp == 0, 2, jnp.where(tp == 1, 4, jnp.where(tp == 2, 8, 16)))
        place = lax.broadcasted_iota(jnp.int32, (total.shape[0], 1), 0) + first_place + 1
        counted = jnp.minimum(place, span).astype(f32)
        diff = (total / counted - runs[0][reach:]).astype(bf16)
        product = jnp.dot(diff, mix[...], preferred_element_type=f32)
        return (product * gain[...]).astype(bf16)

    early = jnp.zeros(halo.shape, bf16)
    pooled[...] = pool_rows(jnp.concatenate([early, pool[...]], axis=0), me * row_count)

    for yy, place in ((1 - y, 0), (y, 1)):
        span = pl.ds(block(yy, 0), 2 * tokens)

        @pl.loop(0, front)
        def _(h):
            part[span, fcols(h)] = jnp.dot(
                pooled[span, :], proj[:, fcols(h)], preferred_element_type=f32
            ).astype(bf16)

        @pl.loop(1, pieces)
        def _(k):
            pair_copy(yy, place, k).start()

    @pl.when(me == 0)
    def _():
        halo[...] = jnp.zeros(halo.shape, bf16)

    @pl.when(me > 0)
    def _():
        halo_copy().wait_recv()

    late = pool_rows(jnp.concatenate([halo[...], pool[:reach, :]], axis=0), me * row_count)

    @pl.loop(0, front)
    def _(h):
        part[:reach, fcols(h)] = jnp.dot(
            late, proj[:, fcols(h)], preferred_element_type=f32
        ).astype(bf16)

    pair_copy(1 - y, 0, 0).start()
    pair_copy(y, 1, 0).start()

    @pl.loop(1, 8)
    def _(q):
        meta_copy(q).start()

    @pl.loop(0, pieces)
    def _(step):
        k = (step + 1) % pieces
        pair_copy(1 - y, 0, k).wait_recv()
        far_out[piece(k)] = (
            part[block_piece(1 - y, c, k)].astype(f32) + pair_in[0, piece(k)].astype(f32)
        ).astype(bf16)
        far_copy(k).start()

    @pl.loop(0, pieces)
    def _(step):
        k = (step + 1) % pieces
        pair_copy(y, 1, k).wait_recv()
        far_copy(k).wait_recv()
        added = (
            part[block_piece(y, c, k)].astype(f32)
            + pair_in[1, piece(k)].astype(f32)
            + far_in[piece(k)].astype(f32)
        ).astype(bf16)
        values = stay[piece(k)].astype(f32) + added.astype(f32)
        mixed[piece(k)] = values
        scale = lax.rsqrt(jnp.mean(values * values, axis=1, keepdims=True) + EPS)
        rows[z, piece(k)] = (values * scale * scales[...]).astype(bf16)
        pass_copy(z, k, z1, ra_send).start()

        @pl.when(mid)
        def _():
            pass_copy(z, k, z2, rb_send).start()

    def picks_of(zt):
        places = meta[zt, y, :experts, :]
        level = lax.broadcasted_iota(jnp.int32, places.shape, 0)
        slot = lax.broadcasted_iota(jnp.int32, (C, tokens), 0).astype(f32)

        def one(expert):
            place = jnp.sum(jnp.where(level == expert, places, 0.0), axis=0, keepdims=True)
            return jnp.where(place[:, :tokens] == slot, 1.0, 0.0)

        return jnp.concatenate([one(me), one(peer_expert)], axis=0).astype(bf16)

    def gather(picks, zt, h):
        found = jnp.dot(picks, rows[zt, :, fcols(h)], preferred_element_type=f32)
        found = found.astype(bf16)
        give[zt, :, fcols(h)] = found[C:]
        xf_copy(zt, h).start()
        slots[zt, spot(x, y), fcols(h)] = found[:C]
        yf_copy(zt, x, h).start()

    def arrive(zt, onward):
        meta_here(zt, y)
        picks = picks_of(zt)

        @pl.loop(0, pieces)
        def _(step):
            k = (step + 1) % pieces
            pass_copy(zt, k, z1, ra_send).wait_recv()
            onward(k)

        @pl.loop(0, front)
        def _(h):
            gather(picks, zt, h)

    def nothing(h):
        pass

    def turn(zt):
        @pl.loop(0, front)
        def _(h):
            xf_copy(zt, h).wait_recv()
            yf_copy(zt, 1 - x, h).start()

    def complete(zt):
        @pl.loop(0, front)
        def _(h):
            yf_copy(zt, x, h).wait_recv()
            yf_copy(zt, 1 - x, h).wait_recv()
            mf_copy(zt, h).start()

    def compute(zt):
        @pl.loop(0, front)
        def _(h):
            mf_copy(zt, h).wait_recv()

        v = slots[zt]
        gate = jnp.dot(v, wg[...], preferred_element_type=f32)
        upper = jnp.dot(v, wu[...], preferred_element_type=f32)
        hidden = (gate * (1.0 / (1.0 + jnp.exp(-gate))) * upper).astype(bf16)

        @pl.loop(0, back)
        def _(h):
            parts[zt, :, bcols(h)] = jnp.dot(
                hidden, wd[:, bcols(h)], preferred_element_type=f32
            ).astype(bf16)
            mb_copy(zt, h).start()

    def pair_sum(zt, far, first=0, stop=back):
        @pl.loop(first, stop)
        def _(h):
            mb_copy(zt, h).wait_recv()
            total = (
                parts[zt, half(c), bcols(h)].astype(f32) + mate_in[zt, :, bcols(h)].astype(f32)
            )
            parts[zt, half(c), bcols(h)] = total.astype(bf16)
            if far:
                yb_copy(zt, 0, h).start()
                yb_copy(zt, 1, h).start()
            else:
                xb_copy(zt, True, h).start()

    def far_piece(zt, h):
        for xx in (0, 1):
            yb_copy(zt, xx, h).wait_recv()
            total = (
                parts[zt, spot(xx, y), bcols(h)].astype(f32)
                + y_in[zt, strip(xx), bcols(h)].astype(f32)
            )
            parts[zt, spot(xx, y), bcols(h)] = total.astype(bf16)
        xb_copy(zt, False, h).start()

    def weights_of(zt, yt):
        places = meta[zt, yt, :experts, :]
        shares = meta[zt, yt, experts:, :]
        level = lax.broadcasted_iota(jnp.int32, places.shape, 0)
        slot = lax.broadcasted_iota(jnp.int32, (C, places.shape[1]), 0).astype(f32)

        def one(expert):
            place = jnp.sum(jnp.where(level == expert, places, 0.0), axis=0, keepdims=True)
            share = jnp.sum(jnp.where(level == expert, shares, 0.0), axis=0, keepdims=True)
            spread = jnp.where(place == slot, share, 0.0)
            head = spread.astype(bf16).astype(f32)
            return head, spread - head

        mine, theirs = one(me), one(peer_expert)
        both = jnp.concatenate([mine[0], theirs[0], mine[1], theirs[1]], axis=0)
        return both.T[:tokens].astype(bf16)

    def blend(spread, zt, yt, h):
        mine = parts[zt, spot(x, yt), bcols(h)]
        theirs = x_in[zt, strip(yt), bcols(h)]
        pair = jnp.concatenate([mine, theirs, mine, theirs], axis=0)
        return jnp.dot(spread, pair, preferred_element_type=f32)

    def near_other(zt, side, first=0, stop=back):
        there = weights_of(zt, 1 - y)

        @pl.loop(first, stop)
        def _(h):
            xb_copy(zt, True, h).wait_recv()
            sums[zt, 1 - y, :, bcols(h)] = blend(there, zt, 1 - y, h).astype(bf16)
            home_copy(zt, 1 - y, side, h).start()

    def near_same(first, stop):
        here = weights_of(z1, y)

        @pl.loop(first, stop)
        def _(h):
            sums[z1, y, :, bcols(h)] = blend(here, z1, y, h).astype(bf16)
            home_copy(z1, y, 0, h).start()

    def merge_same():
        here = weights_of(z2, y)

        @pl.loop(0, back)
        def _(h):
            far_piece(z3, h)
            total = blend(here, z2, y, h)
            line_copy(z2, h, z1).wait_recv()
            sums[z2, y, :, bcols(h)] = (
                total + line_in[z2, :, bcols(h)].astype(f32)
            ).astype(bf16)
            home_copy(z2, y, 1, h).start()

    def far_back():
        mixes[0] = weights_of(z3, y)
        mixes[1] = weights_of(z1, y)

        @pl.loop(0, back + LAG)
        def _(i):
            @pl.when(i < back)
            def _():
                xb_copy(z3, False, i).wait_recv()
                total = blend(mixes[0], z3, y, i)
                line_copy(z3, i, z1).wait_recv()
                sums[z3, y, :, bcols(i)] = (
                    total + line_in[z3, :, bcols(i)].astype(f32)
                ).astype(bf16)
                line_copy(z3, i, z2).start()

            @pl.when(i >= LAG)
            def _():
                k = i - LAG
                total = blend(mixes[1], z1, y, k)
                line_copy(z1, k, z1).wait_recv()
                sums[z1, y, :, bcols(k)] = (
                    total + line_in[z1, :, bcols(k)].astype(f32)
                ).astype(bf16)
                home_copy(z1, y, 0, k).start()

    def far_chain():
        mixes[0] = weights_of(z2, y)
        mixes[1] = weights_of(z3, y)

        @pl.loop(0, 2 * back + LAG)
        def _(i):
            @pl.when(i < 2 * back)
            def _():
                far_piece(z2 + (z3 - z2) * (i // back), i % back)

            @pl.when(i >= LAG)
            def _():
                k = i - LAG
                which, h = k // back, k % back
                zt = z2 + (z3 - z2) * which
                xb_copy(zt, False, h).wait_recv()
                sums[zt, y, :, bcols(h)] = blend(mixes[which], zt, y, h).astype(bf16)
                line_copy(zt, h, z1).start()

    def own_back():
        here = weights_of(z, y)
        there = weights_of(z, 1 - y)

        @pl.loop(0, back)
        def _(h):
            xb_copy(z, True, h).wait_recv()
            sums[z, 1 - y, :, bcols(h)] = blend(there, z, 1 - y, h).astype(bf16)
            mixed[:, bcols(h)] += blend(here, z, y, h)

    def last_send():
        @pl.loop(0, back)
        def _(h):
            home_here(1 - y, 0, h)
            total = (
                sums[z, 1 - y, :, bcols(h)].astype(f32) + home_in[0, 1 - y, :, bcols(h)].astype(f32)
            )

            @pl.when(mid)
            def _():
                home_here(1 - y, 1, h)
                sums[z, 1 - y, :, bcols(h)] = (
                    total + home_in[1, 1 - y, :, bcols(h)].astype(f32)
                ).astype(bf16)

            @pl.when(end)
            def _():
                sums[z, 1 - y, :, bcols(h)] = total.astype(bf16)

            last_copy(h).start()

    def finish():
        @pl.loop(0, back)
        def _(h):
            home_here(y, 0, h)
            last_copy(h).wait_recv()
            total = (
                mixed[:, bcols(h)]
                + home_in[0, y, :, bcols(h)].astype(f32)
                + last_in[:, bcols(h)].astype(f32)
            )

            @pl.when(mid)
            def _():
                home_here(y, 1, h)
                out[:, bcols(h)] = (total + home_in[1, y, :, bcols(h)].astype(f32)).astype(bf16)

            @pl.when(end)
            def _():
                out[:, bcols(h)] = total.astype(bf16)

    def scoped(fn, name):
        def run(*args):
            with jax.named_scope(name):
                fn(*args)
        return run

    arrive = scoped(arrive, "arrive")
    turn = scoped(turn, "turn")
    complete = scoped(complete, "complete")
    compute = scoped(compute, "compute")
    pair_sum = scoped(pair_sum, "pair_sum")
    near_other = scoped(near_other, "near_other")
    near_same = scoped(near_same, "near_same")
    merge_same = scoped(merge_same, "merge_same")
    far_back = scoped(far_back, "far_back")
    own_back = scoped(own_back, "own_back")
    last_send = scoped(last_send, "last_send")
    far_chain = scoped(far_chain, "far_chain")

    def onto(zt, to, send):
        return lambda h: pass_copy(zt, h, to, send).start()

    def first_on(h):
        @pl.when(mid)
        def _():
            pass_copy(z1, h, z2, rb_send).start()

    meta_picks = picks_of(z)

    @pl.loop(0, front)
    def _(h):
        gather(meta_picks, z, h)

    arrive(z1, first_on)

    @pl.when(mid)
    def _():
        arrive(z2, onto(z2, z1, ra_send))

    turn(z1)

    @pl.when(mid)
    def _():
        turn(z2)

    turn(z)

    @pl.when(mid)
    def _():
        arrive(z3, onto(z3, z1, ra_send))

    @pl.when(end)
    def _():
        arrive(z2, nothing)

    for load in loads:
        load.wait()
    complete(z1)
    compute(z1)
    for zt in (z, z1, z2, z3):
        meta_here(zt, 1 - y)

    @pl.when(end)
    def _():
        pair_sum(z1, False, 0, back // 2)
        turn(z2)
        arrive(z3, nothing)
        pair_sum(z1, False, back // 2, back)
        near_other(z1, 0, 0, back // 2)
        near_same(0, back // 2)

    @pl.when(mid)
    def _():
        turn(z3)
        pair_sum(z1, False)

    middle = ((z + 1) // 2) % 2
    second = z + (z2 - z) * middle
    third = z2 + (z - z2) * middle
    complete(second)
    compute(second)

    @pl.when(end)
    def _():
        turn(z3)

    @pl.when(mid)
    def _():
        pair_sum(z2, False)

    complete(third)
    compute(third)

    @pl.when(end)
    def _():
        near_other(z1, 0, back // 2, back)
        near_same(back // 2, back)
        pair_sum(z2, True)
        pair_sum(z, False)

    @pl.when(mid)
    def _():
        near_other(z1, 0)

    complete(z3)
    compute(z3)
    pair_sum(z3, True)

    @pl.when(end)
    def _():
        far_chain()

    @pl.when(mid)
    def _():
        pair_sum(z, False)
        near_other(z2, 1)
        merge_same()

    own_back()
    last_send()

    @pl.when(mid)
    def _():
        far_back()

    with jax.named_scope("finish"):
        finish()

    @pl.loop(1, 8)
    def _(q):
        meta_copy(q).wait_send()

    @pl.when(me < count - 1)
    def _():
        halo_copy().wait_send()

    pair_copy(1 - y, 0, None).wait_send()
    pair_copy(y, 1, None).wait_send()
    far_copy(None).wait_send()
    pass_copy(z, None, z1, ra_send).wait_send()
    for zt in (z, z1, z2, z3):
        xf_copy(zt, None).wait_send()
        yf_copy(zt, 0, None).wait_send()
        yf_copy(zt, 1, None).wait_send()
        mf_copy(zt, None).wait_send()
        mb_copy(zt, None).wait_send()
    xb_copy(z, True, None).wait_send()
    xb_copy(z1, True, None).wait_send()
    xb_copy(z3, False, None).wait_send()
    yb_copy(z3, 0, None).wait_send()
    yb_copy(z3, 1, None).wait_send()
    line_copy(z3, None, z1).wait_send()
    home_copy(z1, 0, 0, None).wait_send()
    home_copy(z1, 1, 0, None).wait_send()
    last_copy(None).wait_send()

    @pl.when(mid)
    def _():
        pass_copy(z, None, z2, rb_send).wait_send()
        pass_copy(z1, None, z2, rb_send).wait_send()
        pass_copy(z2, None, z1, ra_send).wait_send()
        pass_copy(z3, None, z1, ra_send).wait_send()
        xb_copy(z2, True, None).wait_send()
        home_copy(z2, 0, 1, None).wait_send()
        home_copy(z2, 1, 1, None).wait_send()

    @pl.when(end)
    def _():
        xb_copy(z2, False, None).wait_send()
        yb_copy(z2, 0, None).wait_send()
        yb_copy(z2, 1, None).wait_send()
        line_copy(z2, None, z1).wait_send()


FRONT, BACK, LAG = 4, 8, 3


def layer_kernel(
    resid, pool_in, pool_mix, pool_gain, out_proj, norm_gain,
    w_gate, w_up, w_down, routes, route_weight, capacity, experts, slices,
):
    row_count, width = resid.shape
    tokens = row_count // slices
    channels = pool_in.shape[1]
    units = w_gate.shape[2]
    bf16, f32 = jnp.bfloat16, jnp.float32
    dma = pltpu.SemaphoreType.DMA
    C = capacity
    vmem = pltpu.VMEM
    pieces = tokens // 16

    def lanes(*shape, pieces):
        return [dma(shape), dma(shape + (pieces,))]

    return pl.pallas_call(
        functools.partial(moe_kernel, FRONT, BACK, capacity, experts),
        out_shape=jax.ShapeDtypeStruct((tokens, width), bf16),
        in_specs=[pl.BlockSpec(memory_space=pl.ANY)] * 11,
        out_specs=pl.BlockSpec(memory_space=pltpu.VMEM),
        scratch_shapes=[
            vmem((row_count, channels), bf16),
            vmem((channels, channels), bf16),
            vmem((1, channels), f32),
            vmem((channels, width), bf16),
            vmem((1, width), f32),
            vmem((2, row_count), jnp.int32),
            vmem((2, row_count), f32),
            vmem((tokens, width), bf16),
            vmem((2**GROUPS, channels), bf16),
            vmem((row_count, channels), bf16),
            vmem((row_count, width), bf16),
            vmem((2, tokens, width), bf16),
            vmem((tokens, width), bf16),
            vmem((tokens, width), bf16),
            vmem((tokens, width), f32),
            vmem((2 * experts, 128), f32),
            vmem((width, units), bf16),
            vmem((width, units), bf16),
            vmem((units, width), bf16),
            vmem((4, tokens, width), bf16),
            vmem((4, 2, 2 * experts, 128), f32),
            vmem((4, 8 * C, width), bf16),
            vmem((4, C, width), bf16),
            vmem((4, 8 * C, width), bf16),
            vmem((4, 4 * C, width), bf16),
            vmem((4, 2 * C, width), bf16),
            vmem((4, 2 * C, width), bf16),
            vmem((4, 2, tokens, width), bf16),
            vmem((4, tokens, width), bf16),
            vmem((2, 2, tokens, width), bf16),
            vmem((tokens, width), bf16),
            vmem((2, tokens, 4 * C), bf16),
            dma((11,)), dma, dma, dma((2,)), dma((2, pieces)), dma, dma((pieces,)),
            dma((8,)), dma((4, 2)), dma((4, pieces)), dma((4,)), dma((4,)),
        ]
        + lanes(4, pieces=FRONT) + lanes(4, 2, pieces=FRONT) + lanes(4, pieces=FRONT)
        + lanes(4, pieces=BACK) + lanes(4, 2, pieces=BACK) + lanes(4, pieces=BACK)
        + lanes(4, pieces=BACK) + lanes(2, 2, pieces=BACK) + [dma, dma((BACK,))],
        compiler_params=pltpu.CompilerParams(
            collective_id=1, has_side_effects=True, vmem_limit_bytes=63 * 2**20
        ),
        cost_estimate=pl.CostEstimate(
            flops=6 * experts * 4 * C * width * units,
            bytes_accessed=4 * 2 * width * units,
            transcendentals=0,
        ),
        name="moe_exchange",
    )(
        resid, pool_in, pool_mix, pool_gain[None], out_proj, norm_gain[None],
        w_gate, w_up, w_down, routes.T, route_weight.T,
    )


def sum_kernel(count, part, out, pair_in, total, y_in, pp_send, pp_recv, y_send, y_recv):
    me = lax.axis_index("sp")
    tp = lax.axis_index("tp")
    core, y = tp % 2, tp // 2
    mate = y * 2 + (1 - core)
    across = (1 - y) * 2 + core
    pieces = count // 16
    mesh_id = pl.DeviceIdType.MESH
    barrier = pltpu.get_barrier_semaphore()
    for peer in (mate, across):
        pl.semaphore_signal(barrier, inc=1, device_id=(me, peer), device_id_type=mesh_id)
    pl.semaphore_wait(barrier, 2)

    def at(yy, c, k):
        return pl.ds(pl.multiple_of((yy * 2 + c) * count + k * 16, 16), 16)

    def piece(k):
        return pl.ds(pl.multiple_of(k * 16, 16), 16)

    def pair_copy(yy, k, place):
        return pltpu.make_async_remote_copy(
            src_ref=part.at[at(yy, 1 - core, k)], dst_ref=pair_in.at[place, piece(k)],
            send_sem=pp_send.at[place, k], recv_sem=pp_recv.at[place, k],
            device_id=(me, mate), device_id_type=mesh_id,
        )

    def far_copy(k):
        return pltpu.make_async_remote_copy(
            src_ref=total.at[piece(k)], dst_ref=y_in.at[piece(k)],
            send_sem=y_send.at[k], recv_sem=y_recv.at[k],
            device_id=(me, across), device_id_type=mesh_id,
        )

    @pl.loop(0, pieces)
    def _(k):
        pair_copy(1 - y, k, 0).start()

    @pl.loop(0, pieces)
    def _(k):
        pair_copy(y, k, 1).start()

    @pl.loop(0, pieces)
    def _(k):
        pair_copy(1 - y, k, 0).wait_recv()
        total[piece(k)] = (
            part[at(1 - y, core, k)].astype(jnp.float32)
            + pair_in[0, piece(k)].astype(jnp.float32)
        ).astype(jnp.bfloat16)
        far_copy(k).start()

    @pl.loop(0, pieces)
    def _(k):
        pair_copy(y, k, 1).wait_recv()
        far_copy(k).wait_recv()
        out[piece(k)] = (
            part[at(y, core, k)].astype(jnp.float32)
            + pair_in[1, piece(k)].astype(jnp.float32)
            + y_in[piece(k)].astype(jnp.float32)
        ).astype(jnp.bfloat16)

    @pl.loop(0, pieces)
    def _(k):
        pair_copy(1 - y, k, 0).wait_send()
        pair_copy(y, k, 1).wait_send()
        far_copy(k).wait_send()


def scatter_sum(part, slices):
    row_count, width = part.shape
    count = row_count // slices
    pieces = count // 16
    bf16 = jnp.bfloat16
    dma = pltpu.SemaphoreType.DMA
    return pl.pallas_call(
        functools.partial(sum_kernel, count),
        out_shape=jax.ShapeDtypeStruct((count, width), bf16),
        in_specs=[pl.BlockSpec(memory_space=pltpu.VMEM)],
        out_specs=pl.BlockSpec(memory_space=pltpu.VMEM),
        scratch_shapes=[
            pltpu.VMEM((2, count, width), bf16),
            pltpu.VMEM((count, width), bf16),
            pltpu.VMEM((count, width), bf16),
            dma((2, pieces)),
            dma((2, pieces)),
            dma((pieces,)),
            dma((pieces,)),
        ],
        compiler_params=pltpu.CompilerParams(
            collective_id=2, has_side_effects=True, vmem_limit_bytes=24 * 2**20
        ),
        cost_estimate=pl.CostEstimate(flops=0, bytes_accessed=2**25, transcendentals=0),
        name="scatter_sum",
    )(part)


def on_device(
    resid,
    pool_in,
    pool_mix,
    pool_gain,
    out_proj,
    norm_gain,
    w_gate,
    w_up,
    w_down,
    routes,
    route_weight,
):
    token_count, width = resid.shape
    choose = routes.shape[1]
    experts = lax.axis_size("sp")
    slices = lax.axis_size("tp")
    sub_count = token_count // slices
    capacity = max(2, 2 * sub_count * choose // experts)
    whole = experts == 8 and slices == 4 and choose == 2 and token_count % 16 == 0
    if whole and sub_count == 2 * capacity and 4 * capacity == 128:
        return layer_kernel(
            resid, pool_in, pool_mix, pool_gain, out_proj, norm_gain,
            w_gate, w_up, w_down, routes, route_weight, capacity, experts, slices,
        )
    tp_index = lax.axis_index("tp")
    diff = group_diff(pool_in)
    pooled = (jnp.dot(diff, pool_mix[0], preferred_element_type=jnp.float32) * pool_gain).astype(
        jnp.bfloat16
    )
    group_part = rounded(jnp.dot(pooled, out_proj, preferred_element_type=jnp.float32)).astype(
        jnp.bfloat16
    )
    if slices == 4 and sub_count % 16 == 0:
        proj = scatter_sum(group_part, slices).astype(jnp.float32)
    else:
        proj = rounded(
            lax.psum_scatter(group_part, "tp", scatter_dimension=0, tiled=True).astype(jnp.float32)
        )
    first = tp_index * sub_count
    mixed = lax.dynamic_slice_in_dim(resid, first, sub_count, 0).astype(jnp.float32) + proj
    normed = normalize(mixed, norm_gain)
    route_rows = lax.dynamic_slice_in_dim(routes, first, sub_count, 0)
    weight_rows = lax.dynamic_slice_in_dim(route_weight, first, sub_count, 0)
    targets = slot_plan(route_rows, 1, capacity, experts)
    outgoing = fill_slots(normed, targets, experts * capacity)
    outgoing = outgoing.reshape(experts, capacity, width)
    arrived = lax.all_to_all(outgoing, "sp", split_axis=0, concat_axis=0, tiled=True)
    block_rows = lax.all_gather(arrived, "tp", axis=0, tiled=True)
    spread = expert_part(block_rows.reshape(-1, width), w_gate, w_up, w_down).reshape(
        block_rows.shape
    )
    stacked = spread.reshape((slices,) + arrived.shape)
    received = lax.all_to_all(stacked, "tp", split_axis=0, concat_axis=0, tiled=True)
    summed = jnp.sum(received.astype(jnp.float32), axis=0)
    returned = lax.all_to_all(
        summed.astype(jnp.bfloat16), "sp", split_axis=0, concat_axis=0, tiled=True
    )
    moe = collect(returned.reshape(-1, width), targets, weight_rows)
    return (mixed + moe).astype(jnp.bfloat16)


def solution(mesh):
    in_specs = (
        P("sp", None),
        P("sp", "tp"),
        P("tp", None, None),
        P("tp"),
        P("tp", None),
        P(),
        P("sp", None, "tp"),
        P("sp", None, "tp"),
        P("sp", "tp", None),
        P("sp", None),
        P("sp", None),
    )
    out_specs = P(("sp", "tp"), None)
    return jax.shard_map(
        on_device, mesh=mesh, in_specs=in_specs, out_specs=out_specs, check_vma=False
    )
```

```python
import functools

import jax
import jax.numpy as jnp
from jax import lax
from jax.experimental import pallas as pl
from jax.experimental.pallas import tpu as pltpu
from jax.sharding import PartitionSpec as P

GROUPS = 4


EPS = 1e-06


def shifted(x, axis, by):
    count = lax.axis_size(axis)
    pairs = [(i, i + by) for i in range(count) if 0 <= i + by < count]
    return lax.ppermute(x, axis, pairs)


def rounded(value):
    return lax.optimization_barrier(value.astype(jnp.bfloat16)).astype(jnp.float32)


def group_diff(pool_in):
    row_count = pool_in.shape[0]
    reach = 2**GROUPS
    before = shifted(pool_in[row_count - reach :], "sp", 1)
    joined = jnp.concatenate([before, pool_in], axis=0).astype(jnp.float32)
    running = jnp.cumsum(joined, axis=0)
    width = jnp.left_shift(jnp.int32(2), lax.axis_index("tp"))
    lagged = lax.dynamic_slice_in_dim(running, reach - width, row_count, 0)
    total = running[reach:] - lagged
    place = lax.axis_index("sp") * row_count + jnp.arange(row_count, dtype=jnp.int32) + 1
    counted = jnp.minimum(place, width).astype(jnp.float32)
    return (total / counted[:, None] - joined[reach:]).astype(jnp.bfloat16)


def normalize(mixed, norm_gain):
    scale = lax.rsqrt(jnp.mean(mixed * mixed, axis=1, keepdims=True) + EPS)
    return (mixed * scale * norm_gain).astype(jnp.bfloat16)


def slot_plan(route_rows, blocks, capacity, experts):
    row_count, choose = route_rows.shape
    flat_routes = route_rows.reshape(blocks, row_count // blocks * choose)
    onehot = (
        flat_routes[:, :, None] == jnp.arange(experts, dtype=jnp.int32)[None, None, :]
    ).astype(jnp.int32)
    earlier = jnp.cumsum(onehot, axis=1) - onehot
    position = jnp.sum(earlier * onehot, axis=2)
    block_ids = jnp.arange(blocks, dtype=jnp.int32)[:, None]
    return (flat_routes * (blocks * capacity) + block_ids * capacity + position).reshape(-1)


def fill_slots(normed, targets, slot_count):
    row_count, width = normed.shape
    slots = jnp.arange(slot_count, dtype=jnp.int32)[:, None, None]
    picks = jnp.sum((targets.reshape(row_count, -1)[None] == slots).astype(jnp.bfloat16), axis=2)
    return jnp.dot(picks, normed, preferred_element_type=jnp.float32).astype(normed.dtype)


def collect(returned, targets, weights):
    row_count, choose = weights.shape
    slots = jnp.arange(returned.shape[0], dtype=jnp.int32)[None, None, :]
    chosen = targets.reshape(row_count, choose)[:, :, None] == slots
    spread = jnp.sum(jnp.where(chosen, weights[:, :, None], 0.0), axis=1)
    head = lax.reduce_precision(spread, 8, 7)
    tail = spread - head
    both = jnp.concatenate([head, tail], axis=0).astype(jnp.bfloat16)
    product = jnp.dot(both, returned, preferred_element_type=jnp.float32)
    return product[:row_count] + product[row_count:]


def expert_part(inputs, w_gate, w_up, w_down):
    gate = jnp.dot(inputs, w_gate[0], preferred_element_type=jnp.float32)
    upper = jnp.dot(inputs, w_up[0], preferred_element_type=jnp.float32)
    hidden = (jax.nn.silu(gate) * upper).astype(jnp.bfloat16)
    return jnp.dot(hidden, w_down[0], preferred_element_type=jnp.float32).astype(jnp.bfloat16)


def line_plan(z):
    first = z + 1 - 2 * (z % 2)
    second = 2 - z // 2
    third = 3 - 3 * (z // 2)
    return first, second, third


def moe_kernel(
    front, back, capacity, experts,
    resid, pool_in, pool_mix, pool_gain, out_proj, norm_gain,
    wg_hbm, wu_hbm, wd_hbm, routes, shares_in, out,
    pool, mix, gain, proj, scales, named, shares, stay, halo, pooled, part,
    pair_in, far_out, far_in, mixed, meta_in,
    wg, wu, wd, rows, meta, slots, give, parts,
    mate_in, y_in, x_in, sums, line_in, home_in, last_in, mixes,
    w_sem, h_send, h_recv, pp_send, pp_recv, fy_send, fy_recv,
    m_send, m_recv, r_recv, ra_send, rb_send,
    xf_send, xf_recv, yf_send, yf_recv, mf_send, mf_recv,
    mb_send, mb_recv, yb_send, yb_recv, xb_send, xb_recv,
    zf_send, zf_recv, zh_send, zh_recv, yl_send, yl_recv,
):
    me = lax.axis_index("sp")
    tp = lax.axis_index("tp")
    z, x = me // 2, me % 2
    y, c = tp // 2, tp % 2
    C = capacity
    tokens, width = out.shape
    count = lax.axis_size("sp")
    row_count = pool.shape[0]
    reach = halo.shape[0]
    first = pl.multiple_of(tp * tokens, tokens)
    pieces = tokens // 16
    wf, wb = width // front, width // back
    z1, z2, z3 = line_plan(z)
    mid = ((z + 1) // 2) % 2 == 1
    end = ((z + 1) // 2) % 2 == 0
    mate = (me, y * 2 + 1 - c)
    across = (me, (1 - y) * 2 + c)
    peer_expert = me + 1 - 2 * x
    beside = (peer_expert, tp)
    f32, bf16 = jnp.float32, jnp.bfloat16

    def plane(zz):
        return (zz * 2 + x, tp)

    def remote(src, dst, send, recv, to):
        return pltpu.make_async_remote_copy(
            src_ref=src, dst_ref=dst, send_sem=send, recv_sem=recv,
            device_id=to, device_id_type=pl.DeviceIdType.MESH,
        )

    def fcols(h):
        if h is None:
            return pl.ds(0, width)
        return pl.ds(pl.multiple_of(h * wf, wf), wf)

    def bcols(h):
        if h is None:
            return pl.ds(0, width)
        return pl.ds(pl.multiple_of(h * wb, wb), wb)

    def spot(xx, yy):
        return pl.ds(pl.multiple_of(c * 4 * C + xx * 2 * C + yy * C, C), C)

    def both(xx):
        return pl.ds(pl.multiple_of(c * 4 * C + xx * 2 * C, 2 * C), 2 * C)

    def half(cc):
        return pl.ds(pl.multiple_of(cc * 4 * C, 4 * C), 4 * C)

    def strip(yy):
        return pl.ds(pl.multiple_of(yy * C, C), C)

    def meta_copy(q):
        zq, yq = (z + q // 2) % 4, (y + q) % 2
        return remote(meta_in, meta.at[z, y], m_send.at[q], m_recv.at[z, y],
                      (zq * 2 + x, yq * 2 + c))

    def meta_here(zt, yt):
        remote(meta.at[zt, yt], meta.at[zt, yt], m_send.at[0], m_recv.at[zt, yt],
               mate).wait_recv()

    def at(h):
        return 0 if h is None else h

    def piece(k):
        if k is None:
            return pl.ds(0, tokens)
        return pl.ds(pl.multiple_of(k * 16, 16), 16)

    def block(yy, cc):
        return pl.multiple_of((yy * 2 + cc) * tokens, tokens)

    def block_piece(yy, cc, k):
        return pl.ds(pl.multiple_of(block(yy, cc) + k * 16, 16), 16)

    def halo_copy():
        return remote(pool.at[pl.ds(row_count - reach, reach)], halo, h_send, h_recv,
                      (me + 1, tp))

    def pair_copy(yy, place, k):
        if k is None:
            return remote(part.at[pl.ds(block(yy, 1 - c), tokens)], pair_in.at[place],
                          pp_send.at[place], pp_recv.at[place, 0], mate)
        return remote(part.at[block_piece(yy, 1 - c, k)], pair_in.at[place, piece(k)],
                      pp_send.at[place], pp_recv.at[place, k], mate)

    def far_copy(k):
        return remote(far_out.at[piece(k)], far_in.at[piece(k)],
                      fy_send, fy_recv.at[at(k)], across)

    def pass_copy(zt, h, to, send):
        ref = rows.at[zt, piece(h)]
        return remote(ref, ref, send.at[zt], r_recv.at[zt, at(h)], plane(to))

    def xf_copy(zt, h):
        return remote(give.at[zt, :, fcols(h)], slots.at[zt, spot(x, y), fcols(h)],
                      xf_send.at[zt], xf_recv.at[zt, at(h)], beside)

    def yf_copy(zt, xx, h):
        ref = slots.at[zt, spot(xx, y), fcols(h)]
        return remote(ref, ref, yf_send.at[zt, xx], yf_recv.at[zt, xx, at(h)], across)

    def mf_copy(zt, h):
        ref = slots.at[zt, half(c), fcols(h)]
        return remote(ref, ref, mf_send.at[zt], mf_recv.at[zt, at(h)], mate)

    def mb_copy(zt, h):
        return remote(parts.at[zt, half(1 - c), bcols(h)], mate_in.at[zt, :, bcols(h)],
                      mb_send.at[zt], mb_recv.at[zt, at(h)], mate)

    def yb_copy(zt, xx, h):
        return remote(parts.at[zt, spot(xx, 1 - y), bcols(h)], y_in.at[zt, strip(xx), bcols(h)],
                      yb_send.at[zt, xx], yb_recv.at[zt, xx, at(h)], across)

    def xb_copy(zt, near, h):
        if near:
            return remote(parts.at[zt, both(1 - x), bcols(h)], x_in.at[zt, :, bcols(h)],
                          xb_send.at[zt], xb_recv.at[zt, at(h)], beside)
        return remote(parts.at[zt, spot(1 - x, y), bcols(h)], x_in.at[zt, strip(y), bcols(h)],
                      xb_send.at[zt], xb_recv.at[zt, at(h)], beside)

    def line_copy(zt, h, to):
        return remote(sums.at[zt, y, :, bcols(h)], line_in.at[zt, :, bcols(h)],
                      zf_send.at[zt], zf_recv.at[zt, at(h)], plane(to))

    def home_copy(zt, yt, side, h):
        return remote(sums.at[zt, yt, :, bcols(h)], home_in.at[side, yt, :, bcols(h)],
                      zh_send.at[side, yt], zh_recv.at[side, yt, at(h)], plane(zt))

    def home_here(yt, side, h):
        ref = home_in.at[side, yt, :, bcols(h)]
        remote(ref, ref, zh_send.at[side, yt], zh_recv.at[side, yt, at(h)], mate).wait_recv()

    def last_copy(h):
        return remote(sums.at[z, 1 - y, :, bcols(h)], last_in.at[:, bcols(h)],
                      yl_send, yl_recv.at[at(h)], across)

    small = [
        pltpu.make_async_copy(pool_in, pool, w_sem.at[3]),
        pltpu.make_async_copy(routes, named, w_sem.at[4]),
        pltpu.make_async_copy(shares_in, shares, w_sem.at[5]),
        pltpu.make_async_copy(pool_mix.at[0], mix, w_sem.at[6]),
        pltpu.make_async_copy(pool_gain, gain, w_sem.at[7]),
        pltpu.make_async_copy(out_proj, proj, w_sem.at[8]),
        pltpu.make_async_copy(resid.at[pl.ds(first, tokens)], stay, w_sem.at[9]),
        pltpu.make_async_copy(norm_gain, scales, w_sem.at[10]),
    ]
    loads = [
        pltpu.make_async_copy(wg_hbm.at[0], wg, w_sem.at[0]),
        pltpu.make_async_copy(wu_hbm.at[0], wu, w_sem.at[1]),
        pltpu.make_async_copy(wd_hbm.at[0], wd, w_sem.at[2]),
    ]
    for load in small + loads:
        load.start()

    barrier = pltpu.get_barrier_semaphore()
    for peer in (mate, beside):
        pl.semaphore_signal(barrier, inc=1, device_id=peer,
                            device_id_type=pl.DeviceIdType.MESH)

    @pl.when(me > 0)
    def _():
        pl.semaphore_signal(barrier, inc=1, device_id=(me - 1, tp),
                            device_id_type=pl.DeviceIdType.MESH)

    @pl.loop(1, 8)
    def _(q):
        zq, yq = (z + q // 2) % 4, (y + q) % 2
        pl.semaphore_signal(barrier, inc=1, device_id=(zq * 2 + x, yq * 2 + c),
                            device_id_type=pl.DeviceIdType.MESH)

    pl.semaphore_wait(barrier, 9 + (2 * count - 2 - me) // count)
    small[0].wait()

    @pl.when(me < count - 1)
    def _():
        halo_copy().start()

    for load in small[1:]:
        load.wait()

    level = lax.broadcasted_iota(jnp.int32, (experts, row_count), 0)
    one_is, two_is = named[0:1, :] == level, named[1:2, :] == level
    hit = jnp.where(one_is | two_is, 1.0, 0.0)
    share = jnp.where(one_is, shares[0:1, :], 0.0) + jnp.where(two_is, shares[1:2, :], 0.0)
    head = share.astype(bf16).astype(f32)
    stack = jnp.concatenate([hit, head, share - head, hit], axis=0).astype(bf16)
    row = lax.broadcasted_iota(jnp.int32, (row_count, 128), 0)
    lane = lax.broadcasted_iota(jnp.int32, (row_count, 128), 1)
    inside = lane < tokens
    here = jnp.where((row == lane + first) & inside, 1.0, 0.0).astype(bf16)
    ahead = jnp.where((row >= first) & (row < lane + first) & inside, 1.0, 0.0).astype(bf16)
    taken = jnp.dot(stack, here, preferred_element_type=f32)
    before = jnp.dot(stack, ahead, preferred_element_type=f32)
    table = jnp.concatenate(
        [
            jnp.where(taken[:experts] > 0.5, before[:experts], -1.0),
            taken[experts:2 * experts] + taken[2 * experts:3 * experts],
        ],
        axis=0,
    )
    meta_in[...] = table
    meta[z, y] = table

    def pool_rows(joined, first_place):
        runs = [joined.astype(f32)]
        for by in (1, 2, 4, 8):
            runs.append(runs[-1] + pltpu.roll(runs[-1], by, 0))
        total = jnp.where(
            tp == 0, runs[1], jnp.where(tp == 1, runs[2], jnp.where(tp == 2, runs[3], runs[4]))
        )[reach:]
        span = jnp.where(tp == 0, 2, jnp.where(tp == 1, 4, jnp.where(tp == 2, 8, 16)))
        place = lax.broadcasted_iota(jnp.int32, (total.shape[0], 1), 0) + first_place + 1
        counted = jnp.minimum(place, span).astype(f32)
        diff = (total / counted - runs[0][reach:]).astype(bf16)
        product = jnp.dot(diff, mix[...], preferred_element_type=f32)
        return (product * gain[...]).astype(bf16)

    early = jnp.zeros(halo.shape, bf16)
    pooled[...] = pool_rows(jnp.concatenate([early, pool[...]], axis=0), me * row_count)

    for yy, place in ((1 - y, 0), (y, 1)):
        span = pl.ds(block(yy, 0), 2 * tokens)

        @pl.loop(0, front)
        def _(h):
            part[span, fcols(h)] = jnp.dot(
                pooled[span, :], proj[:, fcols(h)], preferred_element_type=f32
            ).astype(bf16)

        @pl.loop(1, pieces)
        def _(k):
            pair_copy(yy, place, k).start()

    @pl.when(me == 0)
    def _():
        halo[...] = jnp.zeros(halo.shape, bf16)

    @pl.when(me > 0)
    def _():
        halo_copy().wait_recv()

    late = pool_rows(jnp.concatenate([halo[...], pool[:reach, :]], axis=0), me * row_count)

    @pl.loop(0, front)
    def _(h):
        part[:reach, fcols(h)] = jnp.dot(
            late, proj[:, fcols(h)], preferred_element_type=f32
        ).astype(bf16)

    pair_copy(1 - y, 0, 0).start()
    pair_copy(y, 1, 0).start()

    @pl.loop(1, 8)
    def _(q):
        meta_copy(q).start()

    @pl.loop(0, pieces)
    def _(step):
        k = (step + 1) % pieces
        pair_copy(1 - y, 0, k).wait_recv()
        far_out[piece(k)] = (
            part[block_piece(1 - y, c, k)].astype(f32) + pair_in[0, piece(k)].astype(f32)
        ).astype(bf16)
        far_copy(k).start()

    @pl.loop(0, pieces)
    def _(step):
        k = (step + 1) % pieces
        pair_copy(y, 1, k).wait_recv()
        far_copy(k).wait_recv()
        added = (
            part[block_piece(y, c, k)].astype(f32)
            + pair_in[1, piece(k)].astype(f32)
            + far_in[piece(k)].astype(f32)
        ).astype(bf16)
        values = stay[piece(k)].astype(f32) + added.astype(f32)
        mixed[piece(k)] = values
        scale = lax.rsqrt(jnp.mean(values * values, axis=1, keepdims=True) + EPS)
        rows[z, piece(k)] = (values * scale * scales[...]).astype(bf16)
        pass_copy(z, k, z1, ra_send).start()

        @pl.when(mid)
        def _():
            pass_copy(z, k, z2, rb_send).start()

    def picks_of(zt):
        places = meta[zt, y, :experts, :]
        level = lax.broadcasted_iota(jnp.int32, places.shape, 0)
        slot = lax.broadcasted_iota(jnp.int32, (C, tokens), 0).astype(f32)

        def one(expert):
            place = jnp.sum(jnp.where(level == expert, places, 0.0), axis=0, keepdims=True)
            return jnp.where(place[:, :tokens] == slot, 1.0, 0.0)

        return jnp.concatenate([one(me), one(peer_expert)], axis=0).astype(bf16)

    def gather(picks, zt, h):
        found = jnp.dot(picks, rows[zt, :, fcols(h)], preferred_element_type=f32)
        found = found.astype(bf16)
        give[zt, :, fcols(h)] = found[C:]
        xf_copy(zt, h).start()
        slots[zt, spot(x, y), fcols(h)] = found[:C]
        yf_copy(zt, x, h).start()

    def arrive(zt, onward):
        meta_here(zt, y)
        picks = picks_of(zt)

        @pl.loop(0, pieces)
        def _(step):
            k = (step + 1) % pieces
            pass_copy(zt, k, z1, ra_send).wait_recv()
            onward(k)

        @pl.loop(0, front)
        def _(h):
            gather(picks, zt, h)

    def nothing(h):
        pass

    def turn(zt):
        @pl.loop(0, front)
        def _(h):
            xf_copy(zt, h).wait_recv()
            yf_copy(zt, 1 - x, h).start()

    def complete(zt):
        @pl.loop(0, front)
        def _(h):
            yf_copy(zt, x, h).wait_recv()
            yf_copy(zt, 1 - x, h).wait_recv()
            mf_copy(zt, h).start()

    def compute(zt):
        @pl.loop(0, front)
        def _(h):
            mf_copy(zt, h).wait_recv()

        v = slots[zt]
        gate = jnp.dot(v, wg[...], preferred_element_type=f32)
        upper = jnp.dot(v, wu[...], preferred_element_type=f32)
        hidden = (gate * (1.0 / (1.0 + jnp.exp(-gate))) * upper).astype(bf16)

        @pl.loop(0, back)
        def _(h):
            parts[zt, :, bcols(h)] = jnp.dot(
                hidden, wd[:, bcols(h)], preferred_element_type=f32
            ).astype(bf16)
            mb_copy(zt, h).start()

    def pair_sum(zt, far, first=0, stop=back):
        @pl.loop(first, stop)
        def _(h):
            mb_copy(zt, h).wait_recv()
            total = (
                parts[zt, half(c), bcols(h)].astype(f32) + mate_in[zt, :, bcols(h)].astype(f32)
            )
            parts[zt, half(c), bcols(h)] = total.astype(bf16)
            if far:
                yb_copy(zt, 0, h).start()
                yb_copy(zt, 1, h).start()
            else:
                xb_copy(zt, True, h).start()

    def far_piece(zt, h):
        for xx in (0, 1):
            yb_copy(zt, xx, h).wait_recv()
            total = (
                parts[zt, spot(xx, y), bcols(h)].astype(f32)
                + y_in[zt, strip(xx), bcols(h)].astype(f32)
            )
            parts[zt, spot(xx, y), bcols(h)] = total.astype(bf16)
        xb_copy(zt, False, h).start()

    def weights_of(zt, yt):
        places = meta[zt, yt, :experts, :]
        shares = meta[zt, yt, experts:, :]
        level = lax.broadcasted_iota(jnp.int32, places.shape, 0)
        slot = lax.broadcasted_iota(jnp.int32, (C, places.shape[1]), 0).astype(f32)

        def one(expert):
            place = jnp.sum(jnp.where(level == expert, places, 0.0), axis=0, keepdims=True)
            share = jnp.sum(jnp.where(level == expert, shares, 0.0), axis=0, keepdims=True)
            spread = jnp.where(place == slot, share, 0.0)
            head = spread.astype(bf16).astype(f32)
            return head, spread - head

        mine, theirs = one(me), one(peer_expert)
        both = jnp.concatenate([mine[0], theirs[0], mine[1], theirs[1]], axis=0)
        return both.T[:tokens].astype(bf16)

    def blend(spread, zt, yt, h):
        mine = parts[zt, spot(x, yt), bcols(h)]
        theirs = x_in[zt, strip(yt), bcols(h)]
        pair = jnp.concatenate([mine, theirs, mine, theirs], axis=0)
        return jnp.dot(spread, pair, preferred_element_type=f32)

    def near_other(zt, side, first=0, stop=back):
        there = weights_of(zt, 1 - y)

        @pl.loop(first, stop)
        def _(h):
            xb_copy(zt, True, h).wait_recv()
            sums[zt, 1 - y, :, bcols(h)] = blend(there, zt, 1 - y, h).astype(bf16)
            home_copy(zt, 1 - y, side, h).start()

    def near_same(first, stop):
        here = weights_of(z1, y)

        @pl.loop(first, stop)
        def _(h):
            sums[z1, y, :, bcols(h)] = blend(here, z1, y, h).astype(bf16)
            home_copy(z1, y, 0, h).start()

    def merge_same():
        here = weights_of(z2, y)

        @pl.loop(0, back)
        def _(h):
            far_piece(z3, h)
            total = blend(here, z2, y, h)
            line_copy(z2, h, z1).wait_recv()
            sums[z2, y, :, bcols(h)] = (
                total + line_in[z2, :, bcols(h)].astype(f32)
            ).astype(bf16)
            home_copy(z2, y, 1, h).start()

    def far_back():
        mixes[0] = weights_of(z3, y)
        mixes[1] = weights_of(z1, y)

        @pl.loop(0, back + LAG)
        def _(i):
            @pl.when(i < back)
            def _():
                xb_copy(z3, False, i).wait_recv()
                total = blend(mixes[0], z3, y, i)
                line_copy(z3, i, z1).wait_recv()
                sums[z3, y, :, bcols(i)] = (
                    total + line_in[z3, :, bcols(i)].astype(f32)
                ).astype(bf16)
                line_copy(z3, i, z2).start()

            @pl.when(i >= LAG)
            def _():
                k = i - LAG
                total = blend(mixes[1], z1, y, k)
                line_copy(z1, k, z1).wait_recv()
                sums[z1, y, :, bcols(k)] = (
                    total + line_in[z1, :, bcols(k)].astype(f32)
                ).astype(bf16)
                home_copy(z1, y, 0, k).start()

    def far_chain():
        mixes[0] = weights_of(z2, y)
        mixes[1] = weights_of(z3, y)

        @pl.loop(0, 2 * back + LAG)
        def _(i):
            @pl.when(i < 2 * back)
            def _():
                far_piece(z2 + (z3 - z2) * (i // back), i % back)

            @pl.when(i >= LAG)
            def _():
                k = i - LAG
                which, h = k // back, k % back
                zt = z2 + (z3 - z2) * which
                xb_copy(zt, False, h).wait_recv()
                sums[zt, y, :, bcols(h)] = blend(mixes[which], zt, y, h).astype(bf16)
                line_copy(zt, h, z1).start()

    def own_back():
        here = weights_of(z, y)
        there = weights_of(z, 1 - y)

        @pl.loop(0, back)
        def _(h):
            xb_copy(z, True, h).wait_recv()
            sums[z, 1 - y, :, bcols(h)] = blend(there, z, 1 - y, h).astype(bf16)
            mixed[:, bcols(h)] += blend(here, z, y, h)

    def last_send():
        @pl.loop(0, back)
        def _(h):
            home_here(1 - y, 0, h)
            total = (
                sums[z, 1 - y, :, bcols(h)].astype(f32) + home_in[0, 1 - y, :, bcols(h)].astype(f32)
            )

            @pl.when(mid)
            def _():
                home_here(1 - y, 1, h)
                sums[z, 1 - y, :, bcols(h)] = (
                    total + home_in[1, 1 - y, :, bcols(h)].astype(f32)
                ).astype(bf16)

            @pl.when(end)
            def _():
                sums[z, 1 - y, :, bcols(h)] = total.astype(bf16)

            last_copy(h).start()

    def finish():
        @pl.loop(0, back)
        def _(h):
            home_here(y, 0, h)
            last_copy(h).wait_recv()
            total = (
                mixed[:, bcols(h)]
                + home_in[0, y, :, bcols(h)].astype(f32)
                + last_in[:, bcols(h)].astype(f32)
            )

            @pl.when(mid)
            def _():
                home_here(y, 1, h)
                out[:, bcols(h)] = (total + home_in[1, y, :, bcols(h)].astype(f32)).astype(bf16)

            @pl.when(end)
            def _():
                out[:, bcols(h)] = total.astype(bf16)

    def scoped(fn, name):
        def run(*args):
            with jax.named_scope(name):
                fn(*args)
        return run

    arrive = scoped(arrive, "arrive")
    turn = scoped(turn, "turn")
    complete = scoped(complete, "complete")
    compute = scoped(compute, "compute")
    pair_sum = scoped(pair_sum, "pair_sum")
    near_other = scoped(near_other, "near_other")
    near_same = scoped(near_same, "near_same")
    merge_same = scoped(merge_same, "merge_same")
    far_back = scoped(far_back, "far_back")
    own_back = scoped(own_back, "own_back")
    last_send = scoped(last_send, "last_send")
    far_chain = scoped(far_chain, "far_chain")

    def onto(zt, to, send):
        return lambda h: pass_copy(zt, h, to, send).start()

    def first_on(h):
        @pl.when(mid)
        def _():
            pass_copy(z1, h, z2, rb_send).start()

    meta_picks = picks_of(z)

    @pl.loop(0, front)
    def _(h):
        gather(meta_picks, z, h)

    arrive(z1, first_on)

    @pl.when(mid)
    def _():
        arrive(z2, onto(z2, z1, ra_send))

    turn(z1)

    @pl.when(mid)
    def _():
        turn(z2)

    turn(z)

    @pl.when(mid)
    def _():
        arrive(z3, onto(z3, z1, ra_send))

    @pl.when(end)
    def _():
        arrive(z2, nothing)

    for load in loads:
        load.wait()
    complete(z1)
    compute(z1)
    for zt in (z, z1, z2, z3):
        meta_here(zt, 1 - y)

    @pl.when(end)
    def _():
        pair_sum(z1, False, 0, back // 2)
        turn(z2)
        arrive(z3, nothing)
        pair_sum(z1, False, back // 2, back)
        near_other(z1, 0, 0, back // 2)
        near_same(0, back // 2)

    @pl.when(mid)
    def _():
        turn(z3)
        pair_sum(z1, False)

    middle = ((z + 1) // 2) % 2
    second = z + (z2 - z) * middle
    third = z2 + (z - z2) * middle
    complete(second)
    compute(second)

    @pl.when(end)
    def _():
        pair_sum(z, False)
        turn(z3)

    @pl.when(mid)
    def _():
        pair_sum(z2, False)

    complete(third)
    compute(third)

    @pl.when(end)
    def _():
        near_other(z1, 0, back // 2, back)
        near_same(back // 2, back)
        pair_sum(z2, True)

    @pl.when(mid)
    def _():
        near_other(z1, 0)

    complete(z3)
    compute(z3)
    pair_sum(z3, True)

    @pl.when(end)
    def _():
        far_chain()

    @pl.when(mid)
    def _():
        pair_sum(z, False)
        near_other(z2, 1)
        merge_same()

    own_back()
    last_send()

    @pl.when(mid)
    def _():
        far_back()

    @pl.loop(1, 8)
    def _(q):
        meta_copy(q).wait_send()

    @pl.when(me < count - 1)
    def _():
        halo_copy().wait_send()

    pair_copy(1 - y, 0, None).wait_send()
    pair_copy(y, 1, None).wait_send()
    far_copy(None).wait_send()
    pass_copy(z, None, z1, ra_send).wait_send()
    for zt in (z, z1, z2, z3):
        xf_copy(zt, None).wait_send()
        yf_copy(zt, 0, None).wait_send()
        yf_copy(zt, 1, None).wait_send()
        mf_copy(zt, None).wait_send()
        mb_copy(zt, None).wait_send()
    xb_copy(z, True, None).wait_send()
    xb_copy(z1, True, None).wait_send()
    xb_copy(z3, False, None).wait_send()
    yb_copy(z3, 0, None).wait_send()
    yb_copy(z3, 1, None).wait_send()

    @pl.when(mid)
    def _():
        pass_copy(z, None, z2, rb_send).wait_send()
        pass_copy(z1, None, z2, rb_send).wait_send()
        pass_copy(z2, None, z1, ra_send).wait_send()
        pass_copy(z3, None, z1, ra_send).wait_send()
        xb_copy(z2, True, None).wait_send()
        home_copy(z2, 0, 1, None).wait_send()
        home_copy(z2, 1, 1, None).wait_send()

    @pl.when(end)
    def _():
        xb_copy(z2, False, None).wait_send()
        yb_copy(z2, 0, None).wait_send()
        yb_copy(z2, 1, None).wait_send()
        line_copy(z2, None, z1).wait_send()

    with jax.named_scope("finish"):
        finish()

    line_copy(z3, None, z1).wait_send()
    home_copy(z1, 0, 0, None).wait_send()
    home_copy(z1, 1, 0, None).wait_send()
    last_copy(None).wait_send()


FRONT, BACK, LAG = 4, 4, 2


def layer_kernel(
    resid, pool_in, pool_mix, pool_gain, out_proj, norm_gain,
    w_gate, w_up, w_down, routes, route_weight, capacity, experts, slices,
):
    row_count, width = resid.shape
    tokens = row_count // slices
    channels = pool_in.shape[1]
    units = w_gate.shape[2]
    bf16, f32 = jnp.bfloat16, jnp.float32
    dma = pltpu.SemaphoreType.DMA
    C = capacity
    vmem = pltpu.VMEM
    pieces = tokens // 16

    def lanes(*shape, pieces):
        return [dma(shape), dma(shape + (pieces,))]

    return pl.pallas_call(
        functools.partial(moe_kernel, FRONT, BACK, capacity, experts),
        out_shape=jax.ShapeDtypeStruct((tokens, width), bf16),
        in_specs=[pl.BlockSpec(memory_space=pl.ANY)] * 11,
        out_specs=pl.BlockSpec(memory_space=pltpu.VMEM),
        scratch_shapes=[
            vmem((row_count, channels), bf16),
            vmem((channels, channels), bf16),
            vmem((1, channels), f32),
            vmem((channels, width), bf16),
            vmem((1, width), f32),
            vmem((2, row_count), jnp.int32),
            vmem((2, row_count), f32),
            vmem((tokens, width), bf16),
            vmem((2**GROUPS, channels), bf16),
            vmem((row_count, channels), bf16),
            vmem((row_count, width), bf16),
            vmem((2, tokens, width), bf16),
            vmem((tokens, width), bf16),
            vmem((tokens, width), bf16),
            vmem((tokens, width), f32),
            vmem((2 * experts, 128), f32),
            vmem((width, units), bf16),
            vmem((width, units), bf16),
            vmem((units, width), bf16),
            vmem((4, tokens, width), bf16),
            vmem((4, 2, 2 * experts, 128), f32),
            vmem((4, 8 * C, width), bf16),
            vmem((4, C, width), bf16),
            vmem((4, 8 * C, width), bf16),
            vmem((4, 4 * C, width), bf16),
            vmem((4, 2 * C, width), bf16),
            vmem((4, 2 * C, width), bf16),
            vmem((4, 2, tokens, width), bf16),
            vmem((4, tokens, width), bf16),
            vmem((2, 2, tokens, width), bf16),
            vmem((tokens, width), bf16),
            vmem((2, tokens, 4 * C), bf16),
            dma((11,)), dma, dma, dma((2,)), dma((2, pieces)), dma, dma((pieces,)),
            dma((8,)), dma((4, 2)), dma((4, pieces)), dma((4,)), dma((4,)),
        ]
        + lanes(4, pieces=FRONT) + lanes(4, 2, pieces=FRONT) + lanes(4, pieces=FRONT)
        + lanes(4, pieces=BACK) + lanes(4, 2, pieces=BACK) + lanes(4, pieces=BACK)
        + lanes(4, pieces=BACK) + lanes(2, 2, pieces=BACK) + [dma, dma((BACK,))],
        compiler_params=pltpu.CompilerParams(
            collective_id=1, has_side_effects=True, vmem_limit_bytes=63 * 2**20
        ),
        cost_estimate=pl.CostEstimate(
            flops=6 * experts * 4 * C * width * units,
            bytes_accessed=4 * 2 * width * units,
            transcendentals=0,
        ),
        name="moe_exchange",
    )(
        resid, pool_in, pool_mix, pool_gain[None], out_proj, norm_gain[None],
        w_gate, w_up, w_down, routes.T, route_weight.T,
    )


def sum_kernel(count, part, out, pair_in, total, y_in, pp_send, pp_recv, y_send, y_recv):
    me = lax.axis_index("sp")
    tp = lax.axis_index("tp")
    core, y = tp % 2, tp // 2
    mate = y * 2 + (1 - core)
    across = (1 - y) * 2 + core
    pieces = count // 16
    mesh_id = pl.DeviceIdType.MESH
    barrier = pltpu.get_barrier_semaphore()
    for peer in (mate, across):
        pl.semaphore_signal(barrier, inc=1, device_id=(me, peer), device_id_type=mesh_id)
    pl.semaphore_wait(barrier, 2)

    def at(yy, c, k):
        return pl.ds(pl.multiple_of((yy * 2 + c) * count + k * 16, 16), 16)

    def piece(k):
        return pl.ds(pl.multiple_of(k * 16, 16), 16)

    def pair_copy(yy, k, place):
        return pltpu.make_async_remote_copy(
            src_ref=part.at[at(yy, 1 - core, k)], dst_ref=pair_in.at[place, piece(k)],
            send_sem=pp_send.at[place, k], recv_sem=pp_recv.at[place, k],
            device_id=(me, mate), device_id_type=mesh_id,
        )

    def far_copy(k):
        return pltpu.make_async_remote_copy(
            src_ref=total.at[piece(k)], dst_ref=y_in.at[piece(k)],
            send_sem=y_send.at[k], recv_sem=y_recv.at[k],
            device_id=(me, across), device_id_type=mesh_id,
        )

    @pl.loop(0, pieces)
    def _(k):
        pair_copy(1 - y, k, 0).start()

    @pl.loop(0, pieces)
    def _(k):
        pair_copy(y, k, 1).start()

    @pl.loop(0, pieces)
    def _(k):
        pair_copy(1 - y, k, 0).wait_recv()
        total[piece(k)] = (
            part[at(1 - y, core, k)].astype(jnp.float32)
            + pair_in[0, piece(k)].astype(jnp.float32)
        ).astype(jnp.bfloat16)
        far_copy(k).start()

    @pl.loop(0, pieces)
    def _(k):
        pair_copy(y, k, 1).wait_recv()
        far_copy(k).wait_recv()
        out[piece(k)] = (
            part[at(y, core, k)].astype(jnp.float32)
            + pair_in[1, piece(k)].astype(jnp.float32)
            + y_in[piece(k)].astype(jnp.float32)
        ).astype(jnp.bfloat16)

    @pl.loop(0, pieces)
    def _(k):
        pair_copy(1 - y, k, 0).wait_send()
        pair_copy(y, k, 1).wait_send()
        far_copy(k).wait_send()


def scatter_sum(part, slices):
    row_count, width = part.shape
    count = row_count // slices
    pieces = count // 16
    bf16 = jnp.bfloat16
    dma = pltpu.SemaphoreType.DMA
    return pl.pallas_call(
        functools.partial(sum_kernel, count),
        out_shape=jax.ShapeDtypeStruct((count, width), bf16),
        in_specs=[pl.BlockSpec(memory_space=pltpu.VMEM)],
        out_specs=pl.BlockSpec(memory_space=pltpu.VMEM),
        scratch_shapes=[
            pltpu.VMEM((2, count, width), bf16),
            pltpu.VMEM((count, width), bf16),
            pltpu.VMEM((count, width), bf16),
            dma((2, pieces)),
            dma((2, pieces)),
            dma((pieces,)),
            dma((pieces,)),
        ],
        compiler_params=pltpu.CompilerParams(
            collective_id=2, has_side_effects=True, vmem_limit_bytes=24 * 2**20
        ),
        cost_estimate=pl.CostEstimate(flops=0, bytes_accessed=2**25, transcendentals=0),
        name="scatter_sum",
    )(part)


def on_device(
    resid,
    pool_in,
    pool_mix,
    pool_gain,
    out_proj,
    norm_gain,
    w_gate,
    w_up,
    w_down,
    routes,
    route_weight,
):
    token_count, width = resid.shape
    choose = routes.shape[1]
    experts = lax.axis_size("sp")
    slices = lax.axis_size("tp")
    sub_count = token_count // slices
    capacity = max(2, 2 * sub_count * choose // experts)
    whole = experts == 8 and slices == 4 and choose == 2 and token_count % 16 == 0
    if whole and sub_count == 2 * capacity and 4 * capacity == 128:
        return layer_kernel(
            resid, pool_in, pool_mix, pool_gain, out_proj, norm_gain,
            w_gate, w_up, w_down, routes, route_weight, capacity, experts, slices,
        )
    tp_index = lax.axis_index("tp")
    diff = group_diff(pool_in)
    pooled = (jnp.dot(diff, pool_mix[0], preferred_element_type=jnp.float32) * pool_gain).astype(
        jnp.bfloat16
    )
    group_part = rounded(jnp.dot(pooled, out_proj, preferred_element_type=jnp.float32)).astype(
        jnp.bfloat16
    )
    if slices == 4 and sub_count % 16 == 0:
        proj = scatter_sum(group_part, slices).astype(jnp.float32)
    else:
        proj = rounded(
            lax.psum_scatter(group_part, "tp", scatter_dimension=0, tiled=True).astype(jnp.float32)
        )
    first = tp_index * sub_count
    mixed = lax.dynamic_slice_in_dim(resid, first, sub_count, 0).astype(jnp.float32) + proj
    normed = normalize(mixed, norm_gain)
    route_rows = lax.dynamic_slice_in_dim(routes, first, sub_count, 0)
    weight_rows = lax.dynamic_slice_in_dim(route_weight, first, sub_count, 0)
    targets = slot_plan(route_rows, 1, capacity, experts)
    outgoing = fill_slots(normed, targets, experts * capacity)
    outgoing = outgoing.reshape(experts, capacity, width)
    arrived = lax.all_to_all(outgoing, "sp", split_axis=0, concat_axis=0, tiled=True)
    block_rows = lax.all_gather(arrived, "tp", axis=0, tiled=True)
    spread = expert_part(block_rows.reshape(-1, width), w_gate, w_up, w_down).reshape(
        block_rows.shape
    )
    stacked = spread.reshape((slices,) + arrived.shape)
    received = lax.all_to_all(stacked, "tp", split_axis=0, concat_axis=0, tiled=True)
    summed = jnp.sum(received.astype(jnp.float32), axis=0)
    returned = lax.all_to_all(
        summed.astype(jnp.bfloat16), "sp", split_axis=0, concat_axis=0, tiled=True
    )
    moe = collect(returned.reshape(-1, width), targets, weight_rows)
    return (mixed + moe).astype(jnp.bfloat16)


def solution(mesh):
    in_specs = (
        P("sp", None),
        P("sp", "tp"),
        P("tp", None, None),
        P("tp"),
        P("tp", None),
        P(),
        P("sp", None, "tp"),
        P("sp", None, "tp"),
        P("sp", "tp", None),
        P("sp", None),
        P("sp", None),
    )
    out_specs = P(("sp", "tp"), None)
    return jax.shard_map(
        on_device, mesh=mesh, in_specs=in_specs, out_specs=out_specs, check_vma=False
    )
```
